512 devices in a mesh: sp: 32 (over z, core), tp: 16 (over y, x).
Axes of the slice: x: 4, y: 4, z: 16, core: 2. Of those that a mesh axis runs over, the one named last changes fastest.
Arguments:
- rec_input: bfloat16 [12288, 3072], P('sp', 'tp'), may hold values from -6 to 6
- gate_input: bfloat16 [12288, 3072], P('sp', 'tp'), may hold values from -6 to 6
- conv_weight: bfloat16 [4, 3072], P(None, 'tp'), may hold values from -3 to 3
- decay_wide: bfloat16 [2, 16, 128, 128], P(None, 'tp'), may hold values from -0.5 to 0.5
- decay_narrow: bfloat16 [2, 16, 64, 64], P(None, 'tp'), may hold values from -0.75 to 0.75
- input_wide: bfloat16 [2, 16, 128, 128], P(None, 'tp'), may hold values from -0.5 to 0.5
- input_narrow: bfloat16 [2, 16, 64, 64], P(None, 'tp'), may hold values from -0.75 to 0.75
- decay_base: float32 [2, 3072], P(None, 'tp'), may hold values from 1.6276042e-06 to 2.0345053e-05
- decay_extra: float32 [2, 12288, 2, 16], P(None, 'sp', None, 'tp'), may hold values from -1 to 0
- tokens: bfloat16 [12288, 2048], P('sp', 'tp'), may hold values from -16 to 16
- out_weight: bfloat16 [3072, 2048], P(None, 'tp'), may hold values from -0.3125 to 0.3125
- norm_gain: float32 [2048], P('tp'), may hold values from 0.1 to 1.9
- shared_gate: bfloat16 [2048, 2048], P(None, 'tp'), may hold values from -0.125 to 0.125
- shared_up: bfloat16 [2048, 2048], P(None, 'tp'), may hold values from -0.125 to 0.125
- shared_down: bfloat16 [2048, 2048], P(None, 'tp'), may hold values from -0.125 to 0.125
- expert_gate: bfloat16 [32, 2048, 2048], P('sp', None, 'tp'), may hold values from -0.125 to 0.125
- expert_up: bfloat16 [32, 2048, 2048], P('sp', None, 'tp'), may hold values from -0.125 to 0.125
- expert_down: bfloat16 [32, 2048, 2048], P('sp', None, 'tp'), may hold values from -0.125 to 0.125
- routes: int32 [12288, 2], P('sp'), may hold values from 0 to 31, all different within a row; in each aligned block of 384 rows (0 to 383, 384 to 767, ...) at most 36 rows name the same one
- route_weight: float32 [12288, 2], P('sp'), may hold values from 0.2 to 1.5
Outputs:
- layer_out: bfloat16 [12288, 2048], P('sp', 'tp')
The draws below stay inside these ranges and needn't reach their ends.
Inputs may be any that keep to these rules, and one draw needn't show every extreme that they name: `routes`: each row names 2 different experts. The rows of one index of sp name no expert more than 36 times, and in some such block one expert exactly 36 times.
All inputs are finite; a program needn't handle non-finite values.
Results may differ from the reference program's by a relative error of at most 0.0052.
Values may be sent and summed in bfloat16 or wider, within the bound.
A program may use at most 64 MiB of HBM per device.

```python
import math
import jax
import jax.numpy as jnp
import numpy as np
from jax import lax

D = 2048
HEADS = 16
HEAD_WIDE = 128
HEAD_NARROW = 64
CONV = 4
FF = 2048
TOP = 2
TOK_DEV = 384
W = 3072
TOKENS = 12288
EXPERTS = 32
CAP = 36
N_SP = 32


def draw_decay_extra(key, part):
    keys = jax.random.split(key, 5)
    slow_share = 0.5
    slow_heads = (jax.random.uniform(keys[0], (2, 1, 2, HEADS)) < slow_share).astype(jnp.float32)
    quick_decay_rate = jax.random.uniform(keys[1], (2, 1, 2, HEADS), minval=0.02, maxval=0.05)
    block_count = TOKENS // TOK_DEV
    block_factor = jnp.exp(jax.random.uniform(keys[2], (2, block_count, 1, 2, HEADS), minval=0.0, maxval=1.1))
    block_factor = jnp.broadcast_to(block_factor, (2, block_count, TOK_DEV, 2, HEADS)).reshape(2, TOKENS, 2, HEADS)
    slow_rate = block_factor * (0.3 / TOKENS)
    surplus_term = -(slow_heads * slow_rate + (1.0 - slow_heads) * quick_decay_rate)
    target_locations = jax.random.randint(keys[3], (3, 2, 1, 2, HEADS), 0, TOKENS)
    extent_list = jnp.log(jax.random.uniform(keys[4], (3, 2, 1, 2, HEADS), minval=0.5, maxval=0.8))
    token_positions = jnp.arange(TOKENS, dtype=jnp.int32)[None, :, None, None]
    for spike_amount in range(3):
        surplus_term = surplus_term + jnp.where(token_positions == target_locations[spike_amount], extent_list[spike_amount], 0.0)
    return surplus_term.astype(jnp.float32)


def draw_tokens(key, part):
    column = jnp.arange(D, dtype=jnp.float32)[None, :]
    scale = 1.0 + 2.0 * column / D
    base = jnp.clip(jax.random.normal(key, (TOKENS, D)), -5.0, 5.0)
    return (base * scale).astype(jnp.bfloat16)


def steps_of(own_key, shape, cuts, smallest, largest):
    factor_of, own = 1.0, jax.random.fold_in(own_key, 6)
    for axis_at, parts in cuts:
        steps = jnp.exp(jax.random.uniform(jax.random.fold_in(own, axis_at), (parts,), jnp.float32, smallest / len(cuts), largest / len(cuts)))
        factor_of = factor_of * jnp.repeat(steps, shape[axis_at] // parts).reshape([-1 if axis == axis_at else 1 for axis in range(len(shape))])
    return factor_of


def assign_block(own_key, own, number, rows, count, top, bound, lean):
    sequence = jax.random.permutation(own_key, count)
    heavy_load, usual = load_shares(count, rows * top, bound, lean, True), load_shares(count, rows * top, bound, lean, False)
    places = jnp.arange(count)

    def named(tallies, turn):
        used = int((tallies > 0).sum())
        fixed = max(1, used // 4)
        moved = fixed + (places - fixed + turn * (used - fixed)) % max(1, count - fixed)
        return jnp.zeros((count,), jnp.int32).at[sequence[jnp.where(places < fixed, places, moved)]].set(jnp.asarray(tallies, jnp.int32))

    tallies = jnp.where(number % 4 == 0, named(heavy_load, number // 4), named(usual, number - number // 4 - 1))
    mixed = jax.random.permutation(jax.random.fold_in(own, 3), count)
    giver, receiver = mixed[0:count // 2 * 2:2], mixed[1:count // 2 * 2:2]
    slack = jnp.minimum(tallies[giver] - 1, bound - tallies[receiver]) // 2
    slack = jnp.where((giver == sequence[0]) | (receiver == sequence[0]) | (tallies[receiver] == 0), 0, jnp.maximum(slack, 0))
    moved = jax.random.randint(jax.random.fold_in(own, 4), (count // 2,), 0, 1 << 20) % (slack + 1)
    tallies = tallies.at[giver].add(-moved).at[receiver].add(moved)
    labels = jnp.searchsorted(jnp.cumsum(tallies), jnp.arange(rows * top), side="right").astype(jnp.int32)
    grid = labels.reshape(top, rows).T
    grid = grid[jax.random.permutation(jax.random.fold_in(own, 1), rows)]
    turn = jax.random.randint(jax.random.fold_in(own, 2), (rows, 1), 0, top)
    return jnp.take_along_axis(grid, (jnp.arange(top)[None, :] + turn) % top, axis=1)


def load_shares(count, total, most, slope, full):
    loads = [(1 << 20) // math.isqrt(standing ** slope) + 1 for standing in range(1, count + 1)]
    largest = most if full else min(most, max(-(-total // count), total * loads[0] // sum(loads)))
    least = 1 if total - largest >= count - 1 else 0
    given, surplus = [largest] + [least] * (count - 1), total - largest - least * (count - 1)
    while surplus > 0:
        free = [i for i in range(1, count) if given[i] < largest] or [i for i in range(1, count) if given[i] < most]
        whole, remaining = sum([loads[i] for i in free]), surplus
        for i in free:
            more = min(most - given[i], max(1, remaining * loads[i] // whole), surplus)
            given[i] = given[i] + more
            surplus = surplus - more
    return np.array(given)


def bell_draw(own_key, extent, deviation, bound, cuts=(), kind=jnp.bfloat16):
    result = deviation * jax.random.normal(own_key, extent, jnp.float32)
    if cuts:
        result = result * steps_of(own_key, extent, cuts, -0.22, 0.18)
    return jnp.clip(result, -bound, bound).astype(kind)


def setup_inputs(seed: int = 0) -> dict:
    arg_keys = jax.random.split(jax.random.key(seed), 21)
    rec_input = bell_draw(arg_keys[0], (TOKENS, W), 1.0, 6.0, ((0, 32), (1, 16)))
    gate_input = bell_draw(arg_keys[1], (TOKENS, W), 1.0, 6.0, ((0, 32), (1, 16)))
    conv_weight = bell_draw(arg_keys[2], (CONV, W), CONV ** -0.5, 3.0, ((1, 16),))
    decay_wide = bell_draw(arg_keys[3], (2, HEADS, HEAD_WIDE, HEAD_WIDE), HEAD_WIDE ** -0.5, 0.5, ((1, 16),))
    decay_narrow = bell_draw(arg_keys[4], (2, HEADS, HEAD_NARROW, HEAD_NARROW), HEAD_NARROW ** -0.5, 0.75, ((1, 16),))
    input_wide = bell_draw(arg_keys[5], (2, HEADS, HEAD_WIDE, HEAD_WIDE), HEAD_WIDE ** -0.5, 0.5, ((1, 16),))
    input_narrow = bell_draw(arg_keys[6], (2, HEADS, HEAD_NARROW, HEAD_NARROW), HEAD_NARROW ** -0.5, 0.75, ((1, 16),))
    decay_base = jnp.clip(jnp.exp(math.log(2.0345052689663135e-05) - 2.5257286 * jax.random.uniform(arg_keys[7], (2, W), jnp.float32) ** steps_of(arg_keys[7], (2, W), ((1, 16),), -0.2, 0.2)), 1.6276042060781037e-06, 2.0345052689663135e-05)
    decay_extra = draw_decay_extra(jax.random.fold_in(arg_keys[20], 71), 0)
    tokens = draw_tokens(jax.random.fold_in(arg_keys[20], 71), 0)
    out_weight = bell_draw(arg_keys[10], (W, D), (W // 9) ** -0.5, 0.3125, ((1, 16),))
    norm_gain = jnp.clip(1.0 + 0.18 * jax.random.normal(arg_keys[11], (D,), jnp.float32), 0.1, 1.9)
    shared_gate = bell_draw(arg_keys[12], (D, FF), D ** -0.5, 0.125, ((1, 16),))
    shared_up = bell_draw(arg_keys[13], (D, FF), D ** -0.5, 0.125, ((1, 16),))
    shared_down = bell_draw(arg_keys[14], (FF, D), FF ** -0.5, 0.125, ((1, 16),))
    expert_gate = bell_draw(arg_keys[15], (EXPERTS, D, FF), D ** -0.5, 0.125, ((0, 32), (2, 16)))
    expert_up = bell_draw(arg_keys[16], (EXPERTS, D, FF), D ** -0.5, 0.125, ((0, 32), (2, 16)))
    expert_down = bell_draw(arg_keys[17], (EXPERTS, FF, D), FF ** -0.5, 0.125, ((0, 32), (2, 16)))
    routes_keys = jax.random.split(jax.random.fold_in(arg_keys[18], 1), TOKENS // TOK_DEV)
    routes_turns = jax.random.permutation(jax.random.fold_in(arg_keys[18], 3), TOKENS // TOK_DEV)
    routes = jax.vmap(lambda own, number: assign_block(jax.random.fold_in(arg_keys[18], 2), own, number, TOK_DEV, EXPERTS, TOP, CAP, 2))(routes_keys, routes_turns).reshape((TOKENS, TOP))
    route_weight = jnp.clip(0.2 + 1.3 * jax.random.uniform(arg_keys[19], (TOKENS, TOP), jnp.float32) ** steps_of(arg_keys[19], (TOKENS, TOP), ((0, 32),), -0.2, 0.2), 0.2, 1.5)
    return {"rec_input": rec_input, "gate_input": gate_input, "conv_weight": conv_weight, "decay_wide": decay_wide, "decay_narrow": decay_narrow, "input_wide": input_wide, "input_narrow": input_narrow, "decay_base": decay_base, "decay_extra": decay_extra, "tokens": tokens, "out_weight": out_weight, "norm_gain": norm_gain, "shared_gate": shared_gate, "shared_up": shared_up, "shared_down": shared_down, "expert_gate": expert_gate, "expert_up": expert_up, "expert_down": expert_down, "routes": routes, "route_weight": route_weight}


NORM_EPS = 1e-06
RATE_SCALE = 8.0

def link(earlier, latter):
    return (earlier[0] * latter[0], latter[0] * earlier[1] + latter[1])

def run_scan(decays, drives, reverse):
    if reverse:
        decays = jnp.flip(decays, 0)
        drives = jnp.flip(drives, 0)
    cumulative, states = lax.associative_scan(link, (decays, drives), axis=0)
    if reverse:
        states = jnp.flip(states, 0)
    return states

def channels_per_head(per_head):
    row_count = per_head.shape[0]
    head_count = per_head.shape[2]
    wide_part = jnp.broadcast_to(per_head[:, 0, :, None], (row_count, head_count, HEAD_WIDE))
    narrow_part = jnp.broadcast_to(per_head[:, 1, :, None], (row_count, head_count, HEAD_NARROW))
    return jnp.concatenate([wide_part, narrow_part], axis=2).reshape(row_count, -1)

def block_gate(grouped, wide_blocks, narrow_blocks):
    wide_in = grouped[:, :, :HEAD_WIDE]
    narrow_in = grouped[:, :, HEAD_WIDE:]
    wide_out = jnp.einsum('thi,hij->thj', wide_in, wide_blocks.astype(jnp.float32))
    narrow_out = jnp.einsum('thi,hij->thj', narrow_in, narrow_blocks.astype(jnp.float32))
    joined = jnp.concatenate([wide_out, narrow_out], axis=2)
    return jax.nn.sigmoid(joined.reshape(grouped.shape[0], -1))

def reference(rec_input, gate_input, conv_weight, decay_wide, decay_narrow, input_wide, input_narrow, decay_base, decay_extra, tokens, out_weight, norm_gain, shared_gate, shared_up, shared_down, expert_gate, expert_up, expert_down, routes, route_weight):
    row_count = rec_input.shape[0]
    padded = jnp.pad(rec_input.astype(jnp.float32), ((2, 1), (0, 0)))
    conv_sum = padded[0:row_count] * conv_weight[0].astype(jnp.float32)
    for tap_index in range(1, CONV):
        conv_sum = conv_sum + padded[tap_index:tap_index + row_count] * conv_weight[tap_index].astype(jnp.float32)
    conv_out = conv_sum.astype(jnp.bfloat16)
    conv_wide = conv_out.astype(jnp.float32)
    grouped = conv_wide.reshape(row_count, HEADS, HEAD_WIDE + HEAD_NARROW)
    summed = jnp.zeros((row_count, W), jnp.float32)
    for direction in range(2):
        rate = block_gate(grouped, decay_wide[direction], decay_narrow[direction])
        admit = block_gate(grouped, input_wide[direction], input_narrow[direction])
        log_decay = -RATE_SCALE * rate * decay_base[direction][None, :] + channels_per_head(decay_extra[direction])
        drives = jnp.sqrt(-jnp.expm1(2.0 * log_decay)) * admit * conv_wide
        summed = summed + run_scan(jnp.exp(log_decay), drives, direction == 1)
    mixed = (summed * jax.nn.gelu(gate_input.astype(jnp.float32))).astype(jnp.bfloat16)
    resid = tokens.astype(jnp.float32) + jnp.dot(mixed, out_weight, preferred_element_type=jnp.float32)
    scale_row = lax.rsqrt(lax.optimization_barrier(jnp.mean(resid * resid, axis=1, keepdims=True)) + NORM_EPS)
    normed = (resid * scale_row * norm_gain[None, :]).astype(jnp.bfloat16)
    shared_expert_hidden = (jax.nn.silu(jnp.dot(normed, shared_gate, preferred_element_type=jnp.float32)) * jnp.dot(normed, shared_up, preferred_element_type=jnp.float32)).astype(jnp.bfloat16)
    shared_out = jnp.dot(shared_expert_hidden, shared_down, preferred_element_type=jnp.float32)
    most_rows = N_SP * CAP

    def expert_step(routed_sum, inputs):
        gate_weights, up_weights, down_weights, expert_id = inputs
        matches = routes == expert_id
        weight_row = lax.optimization_barrier(jnp.sum(jnp.where(matches, route_weight, 0.0), axis=1))
        selected = jnp.any(matches, axis=1)
        row_index = jnp.nonzero(selected, size=most_rows, fill_value=0)[0].astype(jnp.int32)
        live_count = jnp.sum(selected.astype(jnp.int32))
        is_live = jnp.arange(most_rows, dtype=jnp.int32) < live_count
        picked = normed[row_index]
        hidden = (jax.nn.silu(jnp.dot(picked, gate_weights, preferred_element_type=jnp.float32)) * jnp.dot(picked, up_weights, preferred_element_type=jnp.float32)).astype(jnp.bfloat16)
        expert_out = jnp.dot(hidden, down_weights, preferred_element_type=jnp.float32).astype(jnp.bfloat16).astype(jnp.float32)
        weights = jnp.where(is_live, weight_row[row_index], 0.0)
        routed_sum = routed_sum.at[row_index].add(weights[:, None] * expert_out)
        return (routed_sum, None)
    routed_sum, unused = lax.scan(expert_step, jnp.zeros((row_count, D), jnp.float32), (expert_gate, expert_up, expert_down, jnp.arange(EXPERTS, dtype=jnp.int32)))
    return (resid + shared_out + routed_sum).astype(jnp.bfloat16)
```

```python
import functools

import jax
import jax.numpy as jnp
from jax import lax
from jax.experimental import pallas as pl
from jax.experimental.pallas import tpu as pltpu
from jax.sharding import PartitionSpec as P

MESH = pl.DeviceIdType.MESH
BF = jnp.bfloat16
F32 = jnp.float32
D = 2048
NORM_EPS = 1e-06
RATE_SCALE = 8.0
NSP = 32
NTP = 16
TOK = 384
CH = 192
WIDE = 128
STEPS = 48
SLOT = 40
ROWS = NSP * SLOT
PAIR = 72
DENSE = NSP * 36
FAR = DENSE // 2
MIXR = 576


def iota(shape, dim):
    return lax.broadcasted_iota(jnp.int32, shape, dim)


def dot(a, b, ca=1, cb=0):
    return lax.dot_general(a, b, (((ca,), (cb,)), ((), ())), preferred_element_type=F32)


def neg_expm1(u):
    poly = u / 40320.0 + 1.0 / 5040.0
    for c in (720.0, 120.0, 24.0, 6.0, 2.0, 1.0):
        poly = poly * u + 1.0 / c
    return -jnp.where(u > -0.5, poly * u, jnp.exp(u) - 1.0)


def silu(x):
    return x * jax.nn.sigmoid(x)


RECV = {}
for _da in range(4):
    for _db in range(4):
        if (_da, _db) != (0, 0):
            for _q in range(2 if _db == 2 or (_da, _db) == (2, 0) else 1):
                RECV[_da, _db, _q] = len(RECV)


class Gather:
    def __init__(self, buf, base, rows, send, recv):
        self.buf, self.base, self.rows, self.send, self.recv = buf, base, rows, send, recv
        t = lax.axis_index("tp")
        self.x, self.y = lax.rem(t, 4), lax.div(t, 4)
        self.sent = []
        self.count = [0, 0]

    def where(self, h, da, db):
        a, b = (self.x, self.y) if h == 0 else (self.y, self.x)
        a, b = lax.rem(a + (da + 8), 4), lax.rem(b + (db + 8), 4)
        return b * 4 + a if h == 0 else a * 4 + b

    def part(self, h, q):
        half, quarter = self.rows // 2, self.rows // 4
        if q is None:
            return pl.ds(self.base + h * half, half)
        return pl.ds(self.base + h * half + q * quarter, quarter)

    def put(self, h, da, db, q, ta, tb):
        at = self.buf.at[self.where(h, -da, -db), self.part(h, q)]
        c = pltpu.make_async_remote_copy(
            src_ref=at,
            dst_ref=at,
            send_sem=self.send.at[h, self.count[h]],
            recv_sem=self.recv.at[h, RECV[(da + ta) % 4, (db + tb) % 4, q or 0]],
            device_id={"tp": self.where(h, ta, tb)},
            device_id_type=MESH,
        )
        self.count[h] += 1
        c.start()
        self.sent.append(c)

    def wait(self, h, da, db, q=None):
        at = self.buf.at[self.where(h, -da, -db), self.part(h, q)]
        pltpu.make_async_remote_copy(
            src_ref=at,
            dst_ref=at,
            send_sem=self.send.at[h, 0],
            recv_sem=self.recv.at[h, RECV[da, db, q or 0]],
            device_id={"tp": self.where(h, 1, 0)},
            device_id_type=MESH,
        ).wait_recv()

    def start(self):
        for h in range(2):
            for ta, tb in ((1, 0), (-1, 0), (0, 1), (0, -1)):
                self.put(h, 0, 0, None, ta, tb)

    def near(self):
        for h in range(2):
            self.wait(h, 1, 0)
            self.put(h, 1, 0, 0, 1, 0)
            self.put(h, 1, 0, None, 0, 1)
            self.put(h, 1, 0, None, 0, -1)
        for h in range(2):
            self.wait(h, 3, 0)
            self.put(h, 3, 0, 1, -1, 0)
            self.put(h, 3, 0, None, 0, 1)
            self.put(h, 3, 0, None, 0, -1)

    def onward(self, h, da):
        self.wait(h, da, 1)
        self.put(h, da, 1, 0, 0, 1)
        self.wait(h, da, 3)
        self.put(h, da, 3, 1, 0, -1)

    def middle(self):
        for h in range(2):
            self.onward(h, 0)
        for h in range(2):
            self.wait(h, 2, 0, 0)
            self.wait(h, 2, 0, 1)
            self.put(h, 2, 0, None, 0, 1)
            self.put(h, 2, 0, None, 0, -1)
        for da in (1, 3):
            for h in range(2):
                self.onward(h, da)

    def rest(self):
        for h in range(2):
            self.onward(h, 2)
        for da in (0, 1, 3, 2):
            for h in range(2):
                for q in range(2):
                    self.wait(h, da, 2, q)

    def drain(self):
        for c in self.sent:
            c.wait_send()


def kernel(
    rec_ref,
    gate_ref,
    conv_ref,
    dw_ref,
    dn_ref,
    iw_ref,
    in_ref,
    base_ref,
    extra_ref,
    tok_ref,
    outw_ref,
    gain_ref,
    sg_ref,
    su_ref,
    sd_ref,
    eg_ref,
    eu_ref,
    ed_ref,
    routes_ref,
    rw_ref,
    out_ref,
    rp,
    hl,
    hr,
    av,
    bv,
    gp,
    tot,
    car,
    mixb,
    wd,
    ww,
    wsgu,
    wegu,
    wsd,
    wed,
    resid,
    sqb,
    nbuf,
    hsbuf,
    rbuf,
    hrbuf,
    outgo,
    arr,
    back,
    ret,
    pt,
    pk0,
    pk1,
    wsem,
    halo_s,
    halo_r,
    car_s,
    car_r,
    sq_s,
    sq_r,
    go_s,
    go_r,
    re_s,
    re_r,
    *gather_sems,
):
    s, t = lax.axis_index("sp"), lax.axis_index("tp")

    barrier = pltpu.get_barrier_semaphore()

    def greet_sp(k, c):
        pl.semaphore_signal(
            barrier, inc=1, device_id={"sp": lax.rem(s + k, NSP)}, device_id_type=MESH
        )
        return c

    def greet_tp(k, c):
        pl.semaphore_signal(
            barrier, inc=1, device_id={"tp": lax.rem(t + k, NTP)}, device_id_type=MESH
        )
        return c

    lax.fori_loop(1, NSP, greet_sp, 0)
    lax.fori_loop(1, NTP, greet_tp, 0)

    r_i, t_i = iota((TOK, TOK), 0), iota((TOK, TOK), 1)
    order = (t_i == (r_i & 7) * STEPS + (r_i >> 3)).astype(BF)
    rp[pl.ds(16, TOK)] = dot(order, rec_ref[...], 1, 1)

    pl.semaphore_wait(barrier, NSP - 1 + NTP - 1)

    up, down = lax.rem(s + 1, NSP), lax.rem(s + NSP - 1, NSP)
    halo_up = pltpu.make_async_remote_copy(
        src_ref=rp.at[pl.ds(16 + 46 * 8, 16)],
        dst_ref=hl,
        send_sem=halo_s.at[0],
        recv_sem=halo_r.at[0],
        device_id={"sp": up},
        device_id_type=MESH,
    )
    halo_up.start()
    halo_down = pltpu.make_async_remote_copy(
        src_ref=rp.at[pl.ds(16, 8)],
        dst_ref=hr,
        send_sem=halo_s.at[1],
        recv_sem=halo_r.at[1],
        device_id={"sp": down},
        device_id_type=MESH,
    )
    halo_down.start()

    loads = []

    def load(src, dst):
        c = pltpu.make_async_copy(src, dst, wsem.at[len(loads)])
        c.start()
        loads.append(c)

    ww[...] = jnp.zeros_like(ww)
    load(outw_ref.at[:, pl.ds(0, WIDE)], wd)
    load(outw_ref.at[:, pl.ds(WIDE, 64)], ww.at[:, pl.ds(0, 64), pl.ds(0, 128)])
    load(outw_ref.at[:, pl.ds(WIDE, 64)], ww.at[:, pl.ds(64, 64), pl.ds(128, 128)])
    n_out = len(loads)
    load(sg_ref, wsgu.at[:, pl.ds(0, 128)])
    load(su_ref, wsgu.at[:, pl.ds(128, 128)])
    load(sd_ref, wsd)
    n_shared = len(loads)
    load(eg_ref, wegu.at[:, pl.ds(0, 128)])
    load(eu_ref, wegu.at[:, pl.ds(128, 128)])
    load(ed_ref, wed)


    for d in range(2):
        rows = jnp.concatenate(
            [
                jnp.broadcast_to(extra_ref[d, 0], (WIDE, TOK)),
                jnp.broadcast_to(extra_ref[d, 1], (CH - WIDE, TOK)),
            ],
            axis=0,
        )
        high = rows.astype(BF)
        left = rows - high.astype(F32)
        mid = left.astype(BF)
        low = (left - mid.astype(F32)).astype(BF)
        av[d] = (dot(order, high, 1, 1) + dot(order, mid, 1, 1)) + dot(order, low, 1, 1)

    halo_up.wait_recv()
    halo_down.wait_recv()
    sub = iota((8, CH), 0)
    first, last = s == 0, s == NSP - 1
    for k in range(2):
        edge = jnp.where(first, 0.0, hl[pl.ds(k * 8 + 7, 1)])
        rolled = pltpu.roll(rp[pl.ds(16 + (46 + k) * 8, 8)], 1, 0)
        rp[pl.ds(k * 8, 8)] = jnp.where(sub == 0, edge, rolled)
    edge = jnp.where(last, 0.0, hr[pl.ds(0, 1)])
    rolled = pltpu.roll(rp[pl.ds(16, 8)], 7, 0)
    rp[pl.ds(16 + TOK, 8)] = jnp.where(sub == 7, edge, rolled)
    taps = conv_ref[...].astype(F32)

    block = 64
    for i in range(TOK // block):
        r0 = i * block
        conv = rp[pl.ds(r0, block)] * taps[0:1]
        for j in range(1, 4):
            conv = conv + rp[pl.ds(r0 + 8 * j, block)] * taps[j : j + 1]
        conv_b = conv.astype(BF)
        conv_f = conv_b.astype(F32)
        wide, narrow = conv_b[:, :WIDE], conv_b[:, WIDE:]
        for d in range(2):
            rate = jax.nn.sigmoid(
                jnp.concatenate([dot(wide, dw_ref[d]), dot(narrow, dn_ref[d])], axis=1)
            )
            admit = jax.nn.sigmoid(
                jnp.concatenate([dot(wide, iw_ref[d]), dot(narrow, in_ref[d])], axis=1)
            )
            log_decay = -RATE_SCALE * rate * base_ref[d : d + 1] + av[d, pl.ds(r0, block)]
            drive = jnp.sqrt(neg_expm1(2.0 * log_decay)) * admit * conv_f
            av[d, pl.ds(r0, block)] = jnp.exp(log_decay)
            bv[d, pl.ds(r0, block)] = drive

    def scan(i, carry):
        c0, s0, c1, s1 = carry
        f = pl.ds(pl.multiple_of(i * 8, 8), 8)
        g = pl.ds(pl.multiple_of((STEPS - 1 - i) * 8, 8), 8)
        a0, a1 = av[0, f], av[1, g]
        s0, s1 = a0 * s0 + bv[0, f], a1 * s1 + bv[1, g]
        c0, c1 = a0 * c0, a1 * c1
        av[0, f], av[1, g] = c0, c1
        bv[0, f], bv[1, g] = s0, s1
        return c0, s0, c1, s1

    one, zero = jnp.ones((8, CH), F32), jnp.zeros((8, CH), F32)
    c0, s0, c1, s1 = lax.fori_loop(0, STEPS, scan, (one, zero, one, zero), unroll=4)

    def chunks(c, st, sequence):
        g, h = jnp.ones((1, CH), F32), jnp.zeros((1, CH), F32)
        gin, hin = zero, zero
        for k in sequence:
            gin = jnp.where(sub == k, g, gin)
            hin = jnp.where(sub == k, h, hin)
            ck, sk = c[k : k + 1], st[k : k + 1]
            g, h = ck * g, ck * h + sk
        return gin, hin, g, h

    g0, h0, gt0, ht0 = chunks(c0, s0, range(8))
    g1, h1, gt1, ht1 = chunks(c1, s1, range(7, -1, -1))
    tot[0, pl.ds(0, 1)] = gt0
    tot[0, pl.ds(1, 1)] = ht0
    tot[1, pl.ds(0, 1)] = gt1
    tot[1, pl.ds(1, 1)] = ht1

    def carry_copy(k):
        dest = lax.rem(s + k, NSP)
        return pltpu.make_async_remote_copy(
            src_ref=tot.at[(dest < s).astype(jnp.int32)],
            dst_ref=car.at[s],
            send_sem=car_s.at[k],
            recv_sem=car_r.at[s],
            device_id={"sp": dest},
            device_id_type=MESH,
        )

    def carry_start(k, c):
        carry_copy(k).start()
        return c

    lax.fori_loop(1, NSP, carry_start, 0)
    car[s] = jnp.zeros((2, CH), F32)

    gp[...] = jax.nn.gelu(dot(order, gate_ref[...], 1, 1))
    routes = routes_ref[...].astype(F32)
    e0, e1 = routes[0:1], routes[1:2]
    e_i = iota((NSP, TOK), 0).astype(F32)
    hit0, hit1 = e_i == e0, e_i == e1
    named = jnp.where(hit0, 1.0, 0.0) + jnp.where(hit1, 1.0, 0.0)
    rank = dot(named.astype(BF), (r_i < t_i).astype(BF))
    def rel(e):
        k = e - (s - 8).astype(F32)
        k = jnp.where(k < 0.0, k + NSP, k)
        return jnp.where(k >= NSP, k - NSP, k)

    place0 = rel(e0) * SLOT + jnp.sum(jnp.where(hit0, rank, 0.0), axis=0, keepdims=True)
    place1 = rel(e1) * SLOT + jnp.sum(jnp.where(hit1, rank, 0.0), axis=0, keepdims=True)
    for k in range(ROWS // 128):
        s_i = (iota((128, TOK), 0) + k * 128).astype(F32)
        pt[pl.ds(k * 128, 128)] = (
            jnp.where(s_i == place0, 1.0, 0.0) + jnp.where(s_i == place1, 1.0, 0.0)
        ).astype(BF)
    col0 = jnp.transpose(jnp.broadcast_to(place0, (128, TOK)))
    col1 = jnp.transpose(jnp.broadcast_to(place1, (128, TOK)))
    for k in range(ROWS // 128):
        l_i = (iota((TOK, 128), 1) + k * 128).astype(F32)
        pk0[:, pl.ds(k * 128, 128)] = jnp.where(l_i == col0, 1.0, 0.0).astype(BF)
        pk1[:, pl.ds(k * 128, 128)] = jnp.where(l_i == col1, 1.0, 0.0).astype(BF)


    def carry_wait(k, c):
        src = lax.rem(s + k, NSP)
        pltpu.make_async_remote_copy(
            src_ref=tot.at[0],
            dst_ref=car.at[src],
            send_sem=car_s.at[k],
            recv_sem=car_r.at[src],
            device_id={"sp": src},
            device_id_type=MESH,
        ).wait_recv()
        return c

    lax.fori_loop(1, NSP, carry_wait, 0)
    ahead, behind = jnp.zeros((1, CH), F32), jnp.zeros((1, CH), F32)
    for j in range(NSP):
        cj = car[j]
        ahead = jnp.where(j < s, cj[0:1] * ahead + cj[1:2], ahead)
        cj = car[NSP - 1 - j]
        behind = jnp.where(NSP - 1 - j > s, cj[0:1] * behind + cj[1:2], behind)
    x0, x1 = h0 + g0 * ahead, h1 + g1 * behind

    for i in range(STEPS):
        f = pl.ds(i * 8, 8)
        total = (bv[0, f] + av[0, f] * x0) + (bv[1, f] + av[1, f] * x1)
        bv[0, f] = total * gp[f]
    tok_i, row_i = iota((TOK, TOK), 0), iota((TOK, TOK), 1)
    chunk = sum(jnp.where(tok_i >= STEPS * k, 1, 0) for k in range(1, 8))
    back_order = (row_i == (tok_i - chunk * STEPS) * 8 + chunk).astype(BF)
    mixed = dot(back_order, bv[0].astype(BF)).astype(BF)
    c_i, l_i = iota((CH, 128), 0), iota((CH, 128), 1)
    low = ((c_i == l_i + WIDE) & (l_i < 64)).astype(BF)
    high = ((c_i == l_i + 64) & (l_i >= 64)).astype(BF)
    gathers = [
        Gather(buf, base, rows, *gather_sems[2 * k : 2 * k + 2])
        for k, (buf, base, rows) in enumerate(
            (
                (mixb, 0, MIXR),
                (nbuf, 0, TOK),
                (hsbuf, 0, TOK),
                (rbuf, 0, FAR),
                (rbuf, FAR, FAR),
                (hrbuf, 0, FAR),
                (hrbuf, FAR, FAR),
            )
        )
    ]
    gm, gn, gs, r0, r1, f0, f1 = gathers
    mixb[t, pl.ds(0, TOK)] = mixed[:, :WIDE]
    mixb[t, pl.ds(TOK, 192)] = (dot(mixed[:192], low) + dot(mixed[192:], high)).astype(BF)
    gm.start()
    gm.near()
    gm.middle()
    gm.rest()
    for c in loads[:n_out]:
        c.wait()

    lhs = jnp.concatenate([mixb[j, pl.ds(0, TOK)] for j in range(NTP)], axis=1)
    res = tok_ref[...].astype(F32) + dot(lhs, wd[...].reshape(NTP * WIDE, 128))
    lhs = jnp.concatenate([mixb[j, pl.ds(TOK, 192)] for j in range(NTP)], axis=1)
    add = dot(lhs, ww[...].reshape(NTP * WIDE, 256))
    res = res + jnp.concatenate([add[:, :128], add[:, 128:]], axis=0)
    resid[...] = res
    nbuf[t] = (res * gain_ref[...]).astype(BF)
    gn.start()

    sqb[t] = jnp.sum(jnp.transpose(res * res), axis=0, keepdims=True)

    def sq_start(k, c):
        pltpu.make_async_remote_copy(
            src_ref=sqb.at[t],
            dst_ref=sqb.at[t],
            send_sem=sq_s.at[k],
            recv_sem=sq_r.at[t],
            device_id={"tp": lax.rem(t + k, NTP)},
            device_id_type=MESH,
        ).start()
        return c

    def sq_wait(k, c):
        src = lax.rem(t + k, NTP)
        pltpu.make_async_remote_copy(
            src_ref=sqb.at[t],
            dst_ref=sqb.at[src],
            send_sem=sq_s.at[k],
            recv_sem=sq_r.at[src],
            device_id={"tp": src},
            device_id_type=MESH,
        ).wait_recv()
        return c

    lax.fori_loop(1, NTP, sq_start, 0)
    gn.near()
    lax.fori_loop(1, NTP, sq_wait, 0)
    square = sqb[0]
    for j in range(1, NTP):
        square = square + sqb[j]
    scale = lax.rsqrt(square / D + NORM_EPS)
    scale = jnp.transpose(jnp.broadcast_to(scale, (128, TOK)))
    normed = (resid[...] * scale * gain_ref[...]).astype(BF)

    outgo[...] = dot(pt[...], normed).astype(BF)

    def place(k):
        return pl.ds(pl.multiple_of(lax.rem(k + 2 * NSP, NSP) * SLOT, 8), SLOT)

    def go_start(k, c):
        dest = lax.rem(s + k, NSP)
        pltpu.make_async_remote_copy(
            src_ref=outgo.at[place(k + 8)],
            dst_ref=arr.at[place(8 - k)],
            send_sem=go_s.at[k],
            recv_sem=go_r.at[lax.rem(NSP - k, NSP)],
            device_id={"sp": dest},
            device_id_type=MESH,
        ).start()
        return c

    def go_wait(k):
        pltpu.make_async_remote_copy(
            src_ref=outgo.at[place(0)],
            dst_ref=arr.at[place(k + 8)],
            send_sem=go_s.at[k],
            recv_sem=go_r.at[k],
            device_id={"sp": lax.rem(s + k, NSP)},
            device_id_type=MESH,
        ).wait_recv()

    def both_ways(a, b, op):
        def step(k, c):
            op(k, c)
            op(NSP - k, c)
            return c

        lax.fori_loop(a, b, step, 0)

    both_ways(1, 16, go_start)
    go_start(16, 0)
    arr[pl.ds(8 * SLOT, SLOT)] = outgo[pl.ds(8 * SLOT, SLOT)]

    p_i, q_i = iota((PAIR, 2 * SLOT), 0), iota((PAIR, 2 * SLOT), 1)
    skip = jnp.where(p_i >= 36, SLOT - 36, 0)
    squeeze = (q_i == p_i + skip).astype(BF)
    p_i, q_i = iota((2 * SLOT, PAIR), 0), iota((2 * SLOT, PAIR), 1)
    spread = ((p_i == q_i + jnp.where(q_i >= 36, SLOT - 36, 0))).astype(BF)

    def pack(c):
        for k in range(8):
            rows = arr[pl.ds((c * 8 + k) * 2 * SLOT, 2 * SLOT)]
            rbuf[t, pl.ds((c * 8 + k) * PAIR, PAIR)] = dot(squeeze, rows).astype(BF)

    def near_wait(k, c):
        go_wait(k)
        return c

    gn.middle()
    gn.rest()
    for c in loads[n_out:n_shared]:
        c.wait()
    lhs = jnp.concatenate([nbuf[j] for j in range(NTP)], axis=1)
    both = dot(lhs, wsgu[...])
    hsbuf[t] = (silu(both[:, :128] * scale) * (both[:, 128:] * scale)).astype(BF)
    gs.start()
    lax.fori_loop(1, 8, near_wait, 0)
    lax.fori_loop(24, NSP, near_wait, 0)
    pack(0)
    r0.start()
    gs.near()
    r0.near()
    gs.middle()
    lax.fori_loop(8, 24, near_wait, 0)
    pack(1)
    r1.start()
    r0.middle()
    gs.rest()
    r1.near()
    r0.rest()
    for c in loads[n_shared:]:
        c.wait()

    def routed(c):
        def step(i, carry):
            r = pl.ds(pl.multiple_of(c * FAR + i * 192, 8), 192)
            left = jnp.concatenate([rbuf[j, r] for j in range(NTP)], axis=1)
            both = dot(left, wegu[...])
            hrbuf[t, r] = (silu(both[:, :128]) * both[:, 128:]).astype(BF)
            return carry

        lax.fori_loop(0, FAR // 192, step, 0)

    routed(0)
    r1.middle()
    f0.start()
    r1.rest()
    routed(1)
    f1.start()
    f1.near()
    f0.near()
    f1.middle()
    lhs = jnp.concatenate([hsbuf[j] for j in range(NTP)], axis=1)
    resid[...] += dot(lhs, wsd[...])
    f1.rest()

    def re_start(k, c):
        pltpu.make_async_remote_copy(
            src_ref=back.at[place(k + 8)],
            dst_ref=ret.at[place(8 - k)],
            send_sem=re_s.at[k],
            recv_sem=re_r.at[lax.rem(NSP - k, NSP)],
            device_id={"sp": lax.rem(s + k, NSP)},
            device_id_type=MESH,
        ).start()
        return c

    def re_wait(k, c):
        pltpu.make_async_remote_copy(
            src_ref=back.at[place(0)],
            dst_ref=ret.at[place(k + 8)],
            send_sem=re_s.at[k],
            recv_sem=re_r.at[k],
            device_id={"sp": lax.rem(s + k, NSP)},
            device_id_type=MESH,
        ).wait_recv()
        return c

    def down(c):
        left = jnp.concatenate([hrbuf[j, pl.ds(c * FAR, FAR)] for j in range(NTP)], axis=1)
        y = dot(left, wed[...]).astype(BF)
        for k in range(8):
            back[pl.ds((c * 8 + k) * 2 * SLOT, 2 * SLOT)] = dot(
                spread, y[k * PAIR : (k + 1) * PAIR]
            ).astype(BF)

    down(1)
    re_start(16, 0)
    both_ways(9, 16, re_start)
    re_start(8, 0)
    f0.middle()
    f0.rest()
    down(0)
    re_start(24, 0)
    both_ways(1, 8, re_start)
    ret[pl.ds(8 * SLOT, SLOT)] = back[pl.ds(8 * SLOT, SLOT)]

    halo_up.wait_send()
    halo_down.wait_send()
    for g in gathers:
        g.drain()

    def drain_sp(k, c):
        carry_copy(k).wait_send()
        for sem in (go_s, re_s):
            pltpu.make_async_remote_copy(
                src_ref=outgo.at[pl.ds(0, SLOT)],
                dst_ref=ret.at[pl.ds(0, SLOT)],
                send_sem=sem.at[k],
                recv_sem=re_r.at[s],
                device_id={"sp": lax.rem(s + k, NSP)},
                device_id_type=MESH,
            ).wait_send()
        return c

    def drain_tp(k, c):
        pltpu.make_async_remote_copy(
            src_ref=sqb.at[t],
            dst_ref=sqb.at[t],
            send_sem=sq_s.at[k],
            recv_sem=sq_r.at[t],
            device_id={"tp": lax.rem(t + k, NTP)},
            device_id_type=MESH,
        ).wait_send()
        return c

    weights = rw_ref[...]
    w0 = jnp.transpose(jnp.broadcast_to(weights[0:1], (128, TOK)))
    w1 = jnp.transpose(jnp.broadcast_to(weights[1:2], (128, TOK)))
    lax.fori_loop(1, NTP, drain_tp, 0)
    half = ROWS // 2

    def combine(c):
        at = pl.ds(c * half, half)
        got = ret[at]
        return w0 * dot(pk0[:, at], got) + w1 * dot(pk1[:, at], got)

    lax.fori_loop(8, 24, re_wait, 0)
    resid[...] += combine(1)
    lax.fori_loop(1, 8, re_wait, 0)
    lax.fori_loop(24, NSP, re_wait, 0)
    out_ref[...] = (resid[...] + combine(0)).astype(BF)
    lax.fori_loop(1, NSP, drain_sp, 0)


def layer(
    rec_input,
    gate_input,
    conv_weight,
    decay_wide,
    decay_narrow,
    input_wide,
    input_narrow,
    decay_base,
    decay_extra,
    tokens,
    out_weight,
    norm_gain,
    shared_gate,
    shared_up,
    shared_down,
    expert_gate,
    expert_up,
    expert_down,
    routes,
    route_weight,
):
    vmem = pl.BlockSpec(memory_space=pltpu.VMEM)
    hbm = pl.BlockSpec(memory_space=pl.ANY)
    dma = pltpu.SemaphoreType.DMA
    gather_sems = [dma((2, 20)), dma((2, len(RECV)))] * 7
    return pl.pallas_call(
        kernel,
        out_shape=jax.ShapeDtypeStruct((TOK, 128), BF),
        in_specs=[vmem] * 10 + [hbm] + [vmem] + [hbm] * 6 + [vmem] * 2,
        out_specs=vmem,
        scratch_shapes=[
            pltpu.VMEM((TOK + 24, CH), F32),
            pltpu.VMEM((16, CH), F32),
            pltpu.VMEM((8, CH), F32),
            pltpu.VMEM((2, TOK, CH), F32),
            pltpu.VMEM((2, TOK, CH), F32),
            pltpu.VMEM((TOK, CH), F32),
            pltpu.VMEM((2, 2, CH), F32),
            pltpu.VMEM((NSP, 2, CH), F32),
            pltpu.VMEM((NTP, 2 * MIXR, 128), BF),
            pltpu.VMEM((NTP, WIDE, 128), BF),
            pltpu.VMEM((NTP, WIDE, 256), BF),
            pltpu.VMEM((D, 256), BF),
            pltpu.VMEM((D, 256), BF),
            pltpu.VMEM((D, 128), BF),
            pltpu.VMEM((D, 128), BF),
            pltpu.VMEM((TOK, 128), F32),
            pltpu.VMEM((NTP, 1, TOK), F32),
            pltpu.VMEM((NTP, TOK, 128), BF),
            pltpu.VMEM((NTP, TOK, 128), BF),
            pltpu.VMEM((NTP, DENSE, 128), BF),
            pltpu.VMEM((NTP, DENSE, 128), BF),
            pltpu.VMEM((ROWS, 128), BF),
            pltpu.VMEM((ROWS, 128), BF),
            pltpu.VMEM((ROWS, 128), BF),
            pltpu.VMEM((ROWS, 128), BF),
            pltpu.VMEM((ROWS, TOK), BF),
            pltpu.VMEM((TOK, ROWS), BF),
            pltpu.VMEM((TOK, ROWS), BF),
            dma((9,)),
            dma((2,)),
            dma((2,)),
            dma((NSP,)),
            dma((NSP,)),
            dma((NTP,)),
            dma((NTP,)),
            dma((NSP,)),
            dma((NSP,)),
            dma((NSP,)),
            dma((NSP,)),
            *gather_sems,
        ],
        compiler_params=pltpu.CompilerParams(
            collective_id=0, has_side_effects=True, vmem_limit_bytes=60 * 1024 * 1024
        ),
        name="layer",
    )(
        rec_input.T,
        gate_input.T,
        conv_weight,
        decay_wide[:, 0],
        decay_narrow[:, 0],
        input_wide[:, 0],
        input_narrow[:, 0],
        decay_base,
        decay_extra.transpose(0, 2, 3, 1),
        tokens,
        out_weight.reshape(NTP, CH, 128),
        norm_gain.reshape(1, 128),
        shared_gate,
        shared_up,
        shared_down,
        expert_gate[0],
        expert_up[0],
        expert_down[0],
        routes.T,
        route_weight.T,
    )


def solution(mesh):
    return jax.shard_map(
        layer,
        mesh=mesh,
        in_specs=(
            P("sp", "tp"),
            P("sp", "tp"),
            P(None, "tp"),
            P(None, "tp", None, None),
            P(None, "tp", None, None),
            P(None, "tp", None, None),
            P(None, "tp", None, None),
            P(None, "tp"),
            P(None, "sp", None, "tp"),
            P("sp", "tp"),
            P(None, "tp"),
            P("tp"),
            P(None, "tp"),
            P(None, "tp"),
            P(None, "tp"),
            P("sp", None, "tp"),
            P("sp", None, "tp"),
            P("sp", None, "tp"),
            P("sp", None),
            P("sp", None),
        ),
        out_specs=P("sp", "tp"),
        check_vma=False,
    )
```

```python
import functools

import jax
import jax.numpy as jnp
from jax import lax
from jax.experimental import pallas as pl
from jax.experimental.pallas import tpu as pltpu
from jax.sharding import PartitionSpec as P

MESH = pl.DeviceIdType.MESH
BF = jnp.bfloat16
F32 = jnp.float32
D = 2048
NORM_EPS = 1e-06
RATE_SCALE = 8.0
NSP = 32
NTP = 16
TOK = 384
CH = 192
WIDE = 128
STEPS = 48
SLOT = 40
ROWS = NSP * SLOT
PAIR = 72
DENSE = NSP * 36
FAR = DENSE // 2
CHUNK = DENSE // 4
MIXR = 576


def iota(shape, dim):
    return lax.broadcasted_iota(jnp.int32, shape, dim)


def dot(a, b, ca=1, cb=0):
    return lax.dot_general(a, b, (((ca,), (cb,)), ((), ())), preferred_element_type=F32)


def neg_expm1(u):
    poly = u / 40320.0 + 1.0 / 5040.0
    for c in (720.0, 120.0, 24.0, 6.0, 2.0, 1.0):
        poly = poly * u + 1.0 / c
    return -jnp.where(u > -0.5, poly * u, jnp.exp(u) - 1.0)


def silu(x):
    return x * jax.nn.sigmoid(x)


MIX_ORDER = (
    (0, 0, 0, 1, 0), (0, 0, 0, 3, 0), (0, 0, 1, 0, 0), (0, 0, 3, 0, 0), (0, 1, 0, 1, 0),
    (0, 1, 0, 3, 0), (0, 1, 1, 0, 0), (0, 1, 3, 0, 0), (0, 0, 2, 0, 0), (0, 0, 2, 0, 1),
    (0, 0, 1, 1, 0), (0, 0, 1, 3, 0), (0, 0, 3, 1, 0), (0, 1, 1, 1, 0), (0, 0, 3, 3, 0),
    (0, 1, 1, 3, 0), (0, 1, 2, 0, 0), (0, 1, 2, 0, 1), (0, 1, 3, 1, 0), (0, 1, 3, 3, 0),
    (0, 0, 2, 1, 0), (0, 0, 2, 3, 0), (0, 1, 2, 1, 0), (0, 1, 2, 3, 0),
)
ORDER = (
    (0, 0, 0, 1, 0), (0, 0, 0, 3, 0), (0, 0, 1, 0, 0), (0, 0, 3, 0, 0), (0, 1, 0, 1, 0),
    (0, 1, 0, 3, 0), (0, 1, 1, 0, 0), (0, 1, 3, 0, 0), (0, 0, 2, 0, 0), (0, 0, 2, 0, 1),
    (0, 0, 1, 1, 0), (0, 0, 1, 3, 0), (0, 0, 3, 1, 0), (0, 1, 1, 1, 0), (0, 0, 3, 3, 0),
    (0, 1, 1, 3, 0), (0, 1, 2, 0, 0), (0, 1, 2, 0, 1), (0, 1, 3, 1, 0), (0, 1, 3, 3, 0),
    (0, 0, 2, 1, 0), (0, 0, 2, 3, 0), (0, 1, 2, 1, 0), (0, 1, 2, 3, 0), "pack3", "shared",
    (5, 0, 0, 1, 0), (5, 0, 0, 3, 0), (5, 0, 1, 0, 0), (5, 0, 3, 0, 0), (5, 1, 0, 1, 0),
    (5, 1, 0, 3, 0), (5, 1, 1, 0, 0), (5, 1, 3, 0, 0), (1, 0, 0, 1, 0), (1, 0, 0, 3, 0),
    (1, 0, 1, 0, 0), (1, 0, 3, 0, 0), "pack2", (1, 1, 0, 1, 0), (1, 1, 0, 3, 0), (1, 1, 1, 0, 0),
    (1, 1, 3, 0, 0), (5, 0, 2, 0, 0), (5, 0, 2, 0, 1), (5, 0, 1, 1, 0), (5, 0, 1, 3, 0), "pack1",
    (5, 1, 1, 1, 0), (5, 0, 3, 1, 0), (5, 0, 3, 3, 0), (5, 1, 1, 3, 0), (5, 1, 2, 0, 0),
    (5, 1, 2, 0, 1), (5, 1, 3, 1, 0), (5, 1, 3, 3, 0), "pack0", (1, 0, 2, 0, 0), (1, 0, 2, 0, 1),
    "sq2", (1, 0, 1, 1, 0), (1, 0, 1, 3, 0), (4, 0, 1, 0, 0), (4, 0, 3, 0, 0), (4, 1, 0, 1, 0),
    (4, 1, 0, 3, 0), (1, 0, 3, 1, 0), (1, 0, 3, 3, 0), (4, 0, 0, 1, 0), (4, 0, 0, 3, 0),
    (1, 1, 1, 1, 0), (1, 1, 1, 3, 0), (4, 1, 1, 0, 0), (4, 1, 3, 0, 0), (1, 1, 2, 0, 0),
    (1, 1, 2, 0, 1), (1, 1, 3, 1, 0), (1, 1, 3, 3, 0), (5, 0, 2, 1, 0), (5, 0, 2, 3, 0),
    (3, 0, 1, 0, 0), (3, 0, 3, 0, 0), (3, 1, 0, 1, 0), (3, 0, 0, 1, 0), (3, 0, 0, 3, 0),
    (3, 1, 0, 3, 0), (3, 1, 1, 0, 0), (3, 1, 3, 0, 0), (5, 1, 2, 1, 0), (5, 1, 2, 3, 0),
    (2, 0, 0, 1, 0), (2, 0, 0, 3, 0), (2, 0, 1, 0, 0), (2, 0, 3, 0, 0), (2, 1, 1, 0, 0),
    (2, 1, 3, 0, 0), (2, 1, 0, 1, 0), (2, 1, 0, 3, 0), (4, 0, 2, 0, 0), (4, 0, 2, 0, 1),
    (1, 0, 2, 1, 0), (1, 0, 2, 3, 0), (4, 0, 1, 1, 0), (4, 0, 1, 3, 0), (4, 1, 1, 1, 0),
    (4, 1, 1, 3, 0), (4, 0, 3, 1, 0), (4, 0, 3, 3, 0), (4, 1, 3, 1, 0), (4, 1, 3, 3, 0),
    (1, 1, 2, 1, 0), (1, 1, 2, 3, 0), (4, 1, 2, 0, 0), (4, 1, 2, 0, 1), (3, 0, 2, 0, 0),
    (3, 0, 2, 0, 1), (3, 0, 1, 1, 0), (3, 0, 1, 3, 0), (3, 1, 1, 1, 0), (3, 0, 3, 1, 0),
    (3, 0, 3, 3, 0), (3, 1, 1, 3, 0), (3, 1, 3, 1, 0), (3, 1, 2, 0, 0), (3, 1, 2, 0, 1),
    (3, 1, 3, 3, 0), "routed3", (2, 0, 2, 0, 0), (2, 0, 2, 0, 1), (2, 0, 1, 1, 0), (2, 0, 1, 3, 0),
    (2, 1, 1, 1, 0), (2, 1, 1, 3, 0), (2, 0, 3, 1, 0), (2, 0, 3, 3, 0), (2, 1, 3, 1, 0),
    (2, 1, 2, 0, 0), (2, 1, 2, 0, 1), (2, 1, 3, 3, 0), (4, 0, 2, 1, 0), (4, 0, 2, 3, 0), "sdown",
    (4, 1, 2, 1, 0), (4, 1, 2, 3, 0), (3, 0, 2, 1, 0), (3, 0, 2, 3, 0), (3, 1, 2, 3, 0),
    (3, 1, 2, 1, 0), (9, 0, 0, 1, 0), (9, 0, 0, 3, 0), (9, 0, 1, 0, 0), (9, 0, 3, 0, 0),
    (9, 1, 1, 0, 0), (9, 1, 3, 0, 0), (9, 1, 0, 1, 0), (9, 1, 0, 3, 0), (2, 0, 2, 1, 0),
    (2, 0, 2, 3, 0), (2, 1, 2, 3, 0), (2, 1, 2, 1, 0), "routed2", (9, 0, 2, 0, 0), (9, 0, 2, 0, 1),
    "routed1", (9, 0, 1, 1, 0), (9, 0, 1, 3, 0), (9, 1, 1, 1, 0), (9, 1, 1, 3, 0), (9, 0, 3, 1, 0),
    (9, 0, 3, 3, 0), (9, 1, 3, 1, 0), (9, 1, 2, 0, 0), (9, 1, 2, 0, 1), (9, 1, 3, 3, 0), "routed0",
    (8, 0, 0, 1, 0), (8, 0, 0, 3, 0), (8, 0, 1, 0, 0), (8, 0, 3, 0, 0), (8, 1, 0, 1, 0),
    (8, 1, 0, 3, 0), (8, 1, 1, 0, 0), (8, 1, 3, 0, 0), (7, 0, 1, 0, 0), (7, 0, 3, 0, 0),
    (9, 0, 2, 1, 0), (9, 0, 2, 3, 0), (7, 0, 0, 1, 0), (7, 0, 0, 3, 0), (7, 1, 0, 1, 0),
    (7, 1, 0, 3, 0), (7, 1, 1, 0, 0), (7, 1, 3, 0, 0), (9, 1, 2, 3, 0), (9, 1, 2, 1, 0),
    (6, 0, 0, 1, 0), (6, 0, 0, 3, 0), (6, 0, 1, 0, 0), (6, 0, 3, 0, 0), (6, 1, 0, 1, 0),
    (6, 1, 0, 3, 0), (6, 1, 1, 0, 0), (6, 1, 3, 0, 0), (8, 0, 2, 0, 0), (8, 0, 2, 0, 1),
    (8, 0, 1, 1, 0), (8, 0, 1, 3, 0), (8, 1, 1, 1, 0), (8, 1, 1, 3, 0), (8, 0, 3, 1, 0),
    (8, 0, 3, 3, 0), (8, 1, 2, 0, 0), (8, 1, 2, 0, 1), (8, 1, 3, 1, 0), (8, 1, 3, 3, 0),
    (7, 0, 2, 0, 0), (7, 0, 2, 0, 1), (7, 0, 1, 1, 0), (7, 0, 1, 3, 0), (7, 0, 3, 1, 0),
    (7, 0, 3, 3, 0), (7, 1, 1, 1, 0), (7, 1, 1, 3, 0), (7, 1, 3, 1, 0), (7, 1, 3, 3, 0),
    (7, 1, 2, 0, 0), (7, 1, 2, 0, 1), "down3", (6, 0, 2, 0, 0), (6, 0, 2, 0, 1), (6, 0, 1, 1, 0),
    (6, 0, 1, 3, 0), (6, 1, 1, 1, 0), (6, 1, 1, 3, 0), (6, 0, 3, 1, 0), (6, 0, 3, 3, 0),
    (6, 1, 2, 0, 0), (6, 1, 2, 0, 1), (6, 1, 3, 1, 0), (6, 1, 3, 3, 0), (8, 0, 2, 1, 0),
    (8, 0, 2, 3, 0), (8, 1, 2, 1, 0), (8, 1, 2, 3, 0), (7, 0, 2, 1, 0), (7, 0, 2, 3, 0),
    (7, 1, 2, 1, 0), (7, 1, 2, 3, 0), (6, 0, 2, 1, 0), (6, 0, 2, 3, 0), (6, 1, 2, 1, 0),
    (6, 1, 2, 3, 0), "down2", "down1", "down0",
)


RECV = {}
for _da in range(4):
    for _db in range(4):
        if (_da, _db) != (0, 0):
            for _q in range(2 if _db == 2 or (_da, _db) == (2, 0) else 1):
                RECV[_da, _db, _q] = len(RECV)


class Gather:
    def __init__(self, buf, base, rows, send, recv):
        self.buf, self.base, self.rows, self.send, self.recv = buf, base, rows, send, recv
        t = lax.axis_index("tp")
        self.x, self.y = lax.rem(t, 4), lax.div(t, 4)
        self.sent = []
        self.count = [0, 0]
        self.seen = [0, 0]

    def where(self, h, da, db):
        a, b = (self.x, self.y) if h == 0 else (self.y, self.x)
        a, b = lax.rem(a + (da + 8), 4), lax.rem(b + (db + 8), 4)
        return b * 4 + a if h == 0 else a * 4 + b

    def part(self, h, q):
        half, quarter = self.rows // 2, self.rows // 4
        if q is None:
            return pl.ds(self.base + h * half, half)
        return pl.ds(self.base + h * half + q * quarter, quarter)

    def put(self, h, da, db, q, ta, tb):
        at = self.buf.at[self.where(h, -da, -db), self.part(h, q)]
        c = pltpu.make_async_remote_copy(
            src_ref=at,
            dst_ref=at,
            send_sem=self.send.at[h, self.count[h]],
            recv_sem=self.recv.at[h, RECV[(da + ta) % 4, (db + tb) % 4, q or 0]],
            device_id={"tp": self.where(h, ta, tb)},
            device_id_type=MESH,
        )
        self.count[h] += 1
        c.start()
        self.sent.append(c)

    def wait(self, h, da, db, q):
        split = db == 2 or (da, db) == (2, 0)
        at = self.buf.at[self.where(h, -da, -db), self.part(h, q if split else None)]
        pltpu.make_async_remote_copy(
            src_ref=at,
            dst_ref=at,
            send_sem=self.send.at[h, 0],
            recv_sem=self.recv.at[h, RECV[da, db, q or 0]],
            device_id={"tp": self.where(h, 1, 0)},
            device_id_type=MESH,
        ).wait_recv()

    def start(self):
        for h in range(2):
            for ta, tb in ((1, 0), (-1, 0), (0, 1), (0, -1)):
                self.put(h, 0, 0, None, ta, tb)

    def take(self, h, da, db, q):
        self.wait(h, da, db, q)
        if db == 0 and da != 2:
            self.put(h, da, 0, 0 if da == 1 else 1, 2 - da, 0)
        if db == 0:
            self.seen[h] += da == 2
            if da != 2 or self.seen[h] == 2:
                self.put(h, da, 0, None, 0, 1)
                self.put(h, da, 0, None, 0, -1)
        else:
            self.put(h, da, db, 0 if db == 1 else 1, 0, 2 - db)

    def finish(self):
        for da in (0, 1, 3, 2):
            for h in range(2):
                for q in range(2):
                    self.wait(h, da, 2, q)

    def drain(self):
        for c in self.sent:
            c.wait_send()


def kernel(
    rec_ref,
    gate_ref,
    conv_ref,
    dw_ref,
    dn_ref,
    iw_ref,
    in_ref,
    base_ref,
    extra_ref,
    tok_ref,
    outw_ref,
    gain_ref,
    sg_ref,
    su_ref,
    sd_ref,
    eg_ref,
    eu_ref,
    ed_ref,
    routes_ref,
    rw_ref,
    out_ref,
    rp,
    hl,
    hr,
    av,
    bv,
    gp,
    tot,
    car,
    mixb,
    wd,
    ww,
    wsgu,
    wegu,
    wsd,
    wed,
    resid,
    sqb,
    sq2b,
    sc2,
    nbuf,
    hsbuf,
    rbuf,
    hrbuf,
    outgo,
    arr,
    back,
    ret,
    pt,
    pk0,
    pk1,
    wsem,
    halo_s,
    halo_r,
    car_s,
    car_r,
    sq_s,
    sq_r,
    sq2_s,
    sq2_r,
    go_s,
    go_r,
    re_s,
    re_r,
    *gather_sems,
):
    s, t = lax.axis_index("sp"), lax.axis_index("tp")

    barrier = pltpu.get_barrier_semaphore()

    def greet_sp(k, c):
        pl.semaphore_signal(
            barrier, inc=1, device_id={"sp": lax.rem(s + k, NSP)}, device_id_type=MESH
        )
        return c

    def greet_tp(k, c):
        pl.semaphore_signal(
            barrier, inc=1, device_id={"tp": lax.rem(t + k, NTP)}, device_id_type=MESH
        )
        return c

    lax.fori_loop(1, NSP, greet_sp, 0)
    lax.fori_loop(1, NTP, greet_tp, 0)

    r_i, t_i = iota((TOK, TOK), 0), iota((TOK, TOK), 1)
    order = (t_i == (r_i & 7) * STEPS + (r_i >> 3)).astype(BF)
    rp[pl.ds(16, TOK)] = dot(order, rec_ref[...], 1, 1)

    pl.semaphore_wait(barrier, NSP - 1 + NTP - 1)

    up, down = lax.rem(s + 1, NSP), lax.rem(s + NSP - 1, NSP)
    halo_up = pltpu.make_async_remote_copy(
        src_ref=rp.at[pl.ds(16 + 46 * 8, 16)],
        dst_ref=hl,
        send_sem=halo_s.at[0],
        recv_sem=halo_r.at[0],
        device_id={"sp": up},
        device_id_type=MESH,
    )
    halo_up.start()
    halo_down = pltpu.make_async_remote_copy(
        src_ref=rp.at[pl.ds(16, 8)],
        dst_ref=hr,
        send_sem=halo_s.at[1],
        recv_sem=halo_r.at[1],
        device_id={"sp": down},
        device_id_type=MESH,
    )
    halo_down.start()

    loads = []

    def load(src, dst):
        c = pltpu.make_async_copy(src, dst, wsem.at[len(loads)])
        c.start()
        loads.append(c)

    ww[...] = jnp.zeros_like(ww)
    load(outw_ref.at[:, pl.ds(0, WIDE)], wd)
    load(outw_ref.at[:, pl.ds(WIDE, 64)], ww.at[:, pl.ds(0, 64), pl.ds(0, 128)])
    load(outw_ref.at[:, pl.ds(WIDE, 64)], ww.at[:, pl.ds(64, 64), pl.ds(128, 128)])
    n_out = len(loads)
    load(sg_ref, wsgu.at[:, pl.ds(0, 128)])
    load(su_ref, wsgu.at[:, pl.ds(128, 128)])
    load(sd_ref, wsd)
    n_shared = len(loads)
    load(eg_ref, wegu.at[:, pl.ds(0, 128)])
    load(eu_ref, wegu.at[:, pl.ds(128, 128)])
    load(ed_ref, wed)


    for d in range(2):
        rows = jnp.concatenate(
            [
                jnp.broadcast_to(extra_ref[d, 0], (WIDE, TOK)),
                jnp.broadcast_to(extra_ref[d, 1], (CH - WIDE, TOK)),
            ],
            axis=0,
        )
        high = rows.astype(BF)
        left = rows - high.astype(F32)
        mid = left.astype(BF)
        low = (left - mid.astype(F32)).astype(BF)
        av[d] = (dot(order, high, 1, 1) + dot(order, mid, 1, 1)) + dot(order, low, 1, 1)

    halo_up.wait_recv()
    halo_down.wait_recv()
    sub = iota((8, CH), 0)
    first, last = s == 0, s == NSP - 1
    for k in range(2):
        edge = jnp.where(first, 0.0, hl[pl.ds(k * 8 + 7, 1)])
        rolled = pltpu.roll(rp[pl.ds(16 + (46 + k) * 8, 8)], 1, 0)
        rp[pl.ds(k * 8, 8)] = jnp.where(sub == 0, edge, rolled)
    edge = jnp.where(last, 0.0, hr[pl.ds(0, 1)])
    rolled = pltpu.roll(rp[pl.ds(16, 8)], 7, 0)
    rp[pl.ds(16 + TOK, 8)] = jnp.where(sub == 7, edge, rolled)
    taps = conv_ref[...].astype(F32)

    block = 64
    for i in range(TOK // block):
        r0 = i * block
        conv = rp[pl.ds(r0, block)] * taps[0:1]
        for j in range(1, 4):
            conv = conv + rp[pl.ds(r0 + 8 * j, block)] * taps[j : j + 1]
        conv_b = conv.astype(BF)
        conv_f = conv_b.astype(F32)
        wide, narrow = conv_b[:, :WIDE], conv_b[:, WIDE:]
        for d in range(2):
            rate = jax.nn.sigmoid(
                jnp.concatenate([dot(wide, dw_ref[d]), dot(narrow, dn_ref[d])], axis=1)
            )
            admit = jax.nn.sigmoid(
                jnp.concatenate([dot(wide, iw_ref[d]), dot(narrow, in_ref[d])], axis=1)
            )
            log_decay = -RATE_SCALE * rate * base_ref[d : d + 1] + av[d, pl.ds(r0, block)]
            drive = jnp.sqrt(neg_expm1(2.0 * log_decay)) * admit * conv_f
            av[d, pl.ds(r0, block)] = jnp.exp(log_decay)
            bv[d, pl.ds(r0, block)] = drive

    def scan(i, carry):
        c0, s0, c1, s1 = carry
        f = pl.ds(pl.multiple_of(i * 8, 8), 8)
        g = pl.ds(pl.multiple_of((STEPS - 1 - i) * 8, 8), 8)
        a0, a1 = av[0, f], av[1, g]
        s0, s1 = a0 * s0 + bv[0, f], a1 * s1 + bv[1, g]
        c0, c1 = a0 * c0, a1 * c1
        av[0, f], av[1, g] = c0, c1
        bv[0, f], bv[1, g] = s0, s1
        return c0, s0, c1, s1

    one, zero = jnp.ones((8, CH), F32), jnp.zeros((8, CH), F32)
    c0, s0, c1, s1 = lax.fori_loop(0, STEPS, scan, (one, zero, one, zero), unroll=4)

    def chunks(c, st, sequence):
        g, h = jnp.ones((1, CH), F32), jnp.zeros((1, CH), F32)
        gin, hin = zero, zero
        for k in sequence:
            gin = jnp.where(sub == k, g, gin)
            hin = jnp.where(sub == k, h, hin)
            ck, sk = c[k : k + 1], st[k : k + 1]
            g, h = ck * g, ck * h + sk
        return gin, hin, g, h

    g0, h0, gt0, ht0 = chunks(c0, s0, range(8))
    g1, h1, gt1, ht1 = chunks(c1, s1, range(7, -1, -1))
    tot[0, pl.ds(0, 1)] = gt0
    tot[0, pl.ds(1, 1)] = ht0
    tot[1, pl.ds(0, 1)] = gt1
    tot[1, pl.ds(1, 1)] = ht1

    def carry_copy(k):
        dest = lax.rem(s + k, NSP)
        return pltpu.make_async_remote_copy(
            src_ref=tot.at[(dest < s).astype(jnp.int32)],
            dst_ref=car.at[s],
            send_sem=car_s.at[k],
            recv_sem=car_r.at[s],
            device_id={"sp": dest},
            device_id_type=MESH,
        )

    def carry_start(k, c):
        carry_copy(k).start()
        return c

    lax.fori_loop(1, NSP, carry_start, 0)
    car[s] = jnp.zeros((2, CH), F32)

    gp[...] = jax.nn.gelu(dot(order, gate_ref[...], 1, 1))
    routes = routes_ref[...].astype(F32)
    e0, e1 = routes[0:1], routes[1:2]
    e_i = iota((NSP, TOK), 0).astype(F32)
    hit0, hit1 = e_i == e0, e_i == e1
    named = jnp.where(hit0, 1.0, 0.0) + jnp.where(hit1, 1.0, 0.0)
    rank = dot(named.astype(BF), (r_i < t_i).astype(BF))
    def rel(e):
        k = e - s.astype(F32)
        k = jnp.where(k < 0.0, k + NSP, k)
        return jnp.where(k > 16.0, 64.0 - 2.0 * k, jnp.maximum(2.0 * k - 1.0, 0.0))

    place0 = rel(e0) * SLOT + jnp.sum(jnp.where(hit0, rank, 0.0), axis=0, keepdims=True)
    place1 = rel(e1) * SLOT + jnp.sum(jnp.where(hit1, rank, 0.0), axis=0, keepdims=True)
    for k in range(ROWS // 128):
        s_i = (iota((128, TOK), 0) + k * 128).astype(F32)
        pt[pl.ds(k * 128, 128)] = (
            jnp.where(s_i == place0, 1.0, 0.0) + jnp.where(s_i == place1, 1.0, 0.0)
        ).astype(BF)
    col0 = jnp.transpose(jnp.broadcast_to(place0, (128, TOK)))
    col1 = jnp.transpose(jnp.broadcast_to(place1, (128, TOK)))
    for k in range(ROWS // 128):
        l_i = (iota((TOK, 128), 1) + k * 128).astype(F32)
        pk0[:, pl.ds(k * 128, 128)] = jnp.where(l_i == col0, 1.0, 0.0).astype(BF)
        pk1[:, pl.ds(k * 128, 128)] = jnp.where(l_i == col1, 1.0, 0.0).astype(BF)


    def carry_wait(k, c):
        src = lax.rem(s + k, NSP)
        pltpu.make_async_remote_copy(
            src_ref=tot.at[0],
            dst_ref=car.at[src],
            send_sem=car_s.at[k],
            recv_sem=car_r.at[src],
            device_id={"sp": src},
            device_id_type=MESH,
        ).wait_recv()
        return c

    lax.fori_loop(1, NSP, carry_wait, 0)
    ahead, behind = jnp.zeros((1, CH), F32), jnp.zeros((1, CH), F32)
    for j in range(NSP):
        cj = car[j]
        ahead = jnp.where(j < s, cj[0:1] * ahead + cj[1:2], ahead)
        cj = car[NSP - 1 - j]
        behind = jnp.where(NSP - 1 - j > s, cj[0:1] * behind + cj[1:2], behind)
    x0, x1 = h0 + g0 * ahead, h1 + g1 * behind

    for i in range(STEPS):
        f = pl.ds(i * 8, 8)
        total = (bv[0, f] + av[0, f] * x0) + (bv[1, f] + av[1, f] * x1)
        bv[0, f] = total * gp[f]
    tok_i, row_i = iota((TOK, TOK), 0), iota((TOK, TOK), 1)
    chunk = sum(jnp.where(tok_i >= STEPS * k, 1, 0) for k in range(1, 8))
    back_order = (row_i == (tok_i - chunk * STEPS) * 8 + chunk).astype(BF)
    mixed = dot(back_order, bv[0].astype(BF)).astype(BF)
    c_i, l_i = iota((CH, 128), 0), iota((CH, 128), 1)
    low = ((c_i == l_i + WIDE) & (l_i < 64)).astype(BF)
    high = ((c_i == l_i + 64) & (l_i >= 64)).astype(BF)
    gathers = [
        Gather(buf, base, rows, *gather_sems[2 * k : 2 * k + 2])
        for k, (buf, base, rows) in enumerate(
            (
                (mixb, 0, MIXR),
                (nbuf, 0, TOK),
                (hsbuf, 0, TOK),
                *((b, c * CHUNK, CHUNK) for b in (rbuf, hrbuf) for c in range(4)),
            )
        )
    ]
    gm, gn, gs = gathers[:3]
    gr, gf = gathers[3:7], gathers[7:]
    mixb[t, pl.ds(0, TOK)] = mixed[:, :WIDE]
    mixb[t, pl.ds(TOK, 192)] = (dot(mixed[:192], low) + dot(mixed[192:], high)).astype(BF)
    gm.start()
    for _, *way in MIX_ORDER:
        gm.take(*way)
    gm.finish()
    for c in loads[:n_out]:
        c.wait()

    lhs = jnp.concatenate([mixb[j, pl.ds(0, TOK)] for j in range(NTP)], axis=1)
    res = tok_ref[...].astype(F32) + dot(lhs, wd[...].reshape(NTP * WIDE, 128))
    lhs = jnp.concatenate([mixb[j, pl.ds(TOK, 192)] for j in range(NTP)], axis=1)
    add = dot(lhs, ww[...].reshape(NTP * WIDE, 256))
    res = res + jnp.concatenate([add[:, :128], add[:, 128:]], axis=0)
    resid[...] = res
    nbuf[t] = (res * gain_ref[...]).astype(BF)
    gn.start()

    outgo[...] = dot(pt[...], nbuf[t]).astype(BF)

    def place(p):
        return pl.ds(pl.multiple_of(p * SLOT, 8), SLOT)

    def both_ways(a, b, op):
        def step(m, c):
            op(2 * m - 1, 2 * m, m)
            op(2 * m, 2 * m - 1, -m)
            return c

        lax.fori_loop(a, b, step, 0)

    def exchange(src, dst, send, recv):
        def copy(p, q, k):
            return pltpu.make_async_remote_copy(
                src_ref=src.at[place(p)],
                dst_ref=dst.at[place(q)],
                send_sem=send.at[p],
                recv_sem=recv.at[q],
                device_id={"sp": lax.rem(s + k + NSP, NSP)},
                device_id_type=MESH,
            )

        return copy

    go, re = exchange(outgo, arr, go_s, go_r), exchange(back, ret, re_s, re_r)
    go(31, 31, 16).start()

    def go_start(i, c):
        m = 16 - i
        go(2 * m, 2 * m - 1, -m).start()
        go(2 * m - 1, 2 * m, m).start()
        return c

    lax.fori_loop(1, 16, go_start, 0)
    arr[pl.ds(0, SLOT)] = outgo[pl.ds(0, SLOT)]

    def arrived(copy, a, b):
        def step(p, c):
            copy(p, p, 1).wait_recv()
            return c

        lax.fori_loop(a, b, step, 0)

    def spread_sums(buf, send, recv):
        def step(k, c):
            pltpu.make_async_remote_copy(
                src_ref=buf.at[t],
                dst_ref=buf.at[t],
                send_sem=send.at[k],
                recv_sem=recv.at[t],
                device_id={"tp": lax.rem(t + k, NTP)},
                device_id_type=MESH,
            ).start()
            return c

        lax.fori_loop(1, NTP, step, 0)

    def total_scale(buf, send, recv):
        def step(k, c):
            src = lax.rem(t + k, NTP)
            pltpu.make_async_remote_copy(
                src_ref=buf.at[t],
                dst_ref=buf.at[src],
                send_sem=send.at[k],
                recv_sem=recv.at[src],
                device_id={"tp": src},
                device_id_type=MESH,
            ).wait_recv()
            return c

        lax.fori_loop(1, NTP, step, 0)
        square = buf[0]
        for j in range(1, NTP):
            square = square + buf[j]
        root = lax.rsqrt(square / D + NORM_EPS)
        return jnp.transpose(jnp.broadcast_to(root, (128, root.shape[1])))

    sqb[t] = jnp.sum(jnp.transpose(res * res), axis=0, keepdims=True)
    spread_sums(sqb, sq_s, sq_r)

    p_i, q_i = iota((PAIR, 2 * SLOT), 0), iota((PAIR, 2 * SLOT), 1)
    squeeze = (q_i == p_i + jnp.where(p_i >= 36, SLOT - 36, 0)).astype(BF)
    p_i, q_i = iota((2 * SLOT, PAIR), 0), iota((2 * SLOT, PAIR), 1)
    spread = (p_i == q_i + jnp.where(q_i >= 36, SLOT - 36, 0)).astype(BF)

    def pack(c):
        arrived(go, max(c * 8, 1), c * 8 + 8)
        for k in range(4):
            rows = arr[pl.ds((c * 4 + k) * 2 * SLOT, 2 * SLOT)]
            rbuf[t, pl.ds((c * 4 + k) * PAIR, PAIR)] = dot(squeeze, rows).astype(BF)
        gr[c].start()

    def squares():
        mine = rbuf[t].astype(F32) / gain_ref[...]
        sq2b[t] = jnp.sum(jnp.transpose(mine * mine), axis=0, keepdims=True)
        spread_sums(sq2b, sq2_s, sq2_r)

    def shared():
        gn.finish()
        scale = total_scale(sqb, sq_s, sq_r)
        for c in loads[n_out:n_shared]:
            c.wait()
        lhs = jnp.concatenate([nbuf[j] for j in range(NTP)], axis=1)
        both = dot(lhs, wsgu[...])
        hsbuf[t] = (silu(both[:, :128] * scale) * (both[:, 128:] * scale)).astype(BF)
        gs.start()

    scaled = []

    def routed(c):
        gr[c].finish()
        if not scaled:
            sc2[...] = total_scale(sq2b, sq2_s, sq2_r)
            for w in loads[n_shared:]:
                w.wait()
            scaled.append(c)

        def step(i, carry):
            r = pl.ds(pl.multiple_of(c * CHUNK + i * (CHUNK // 2), 8), CHUNK // 2)
            left = jnp.concatenate([rbuf[j, r] for j in range(NTP)], axis=1)
            both = dot(left, wegu[...])
            sc = sc2[r]
            hrbuf[t, r] = (silu(both[:, :128] * sc) * (both[:, 128:] * sc)).astype(BF)
            return carry

        lax.fori_loop(0, 2, step, 0)
        gf[c].start()

    def shared_down():
        gs.finish()
        lhs = jnp.concatenate([hsbuf[j] for j in range(NTP)], axis=1)
        resid[...] += dot(lhs, wsd[...])

    def down(c):
        gf[c].finish()
        left = jnp.concatenate([hrbuf[j, pl.ds(c * CHUNK, CHUNK)] for j in range(NTP)], axis=1)
        y = dot(left, wed[...]).astype(BF)
        for k in range(4):
            back[pl.ds((c * 4 + k) * 2 * SLOT, 2 * SLOT)] = dot(
                spread, y[k * PAIR : (k + 1) * PAIR]
            ).astype(BF)

    def give(c):
        if c == 3:
            re(31, 31, 16).start()
        else:
            re(8 * c + 7, 8 * c + 8, 4 * c + 4).start()
        both_ways(4 * c + 1, 4 * c + 4, lambda p, q, k: re(p, q, k).start())
        if c:
            re(8 * c, 8 * c - 1, -4 * c).start()

    for step in ORDER:
        if not isinstance(step, str):
            gathers[step[0] + 1].take(*step[1:])
        elif step == "shared":
            shared()
        elif step == "sdown":
            shared_down()
        elif step == "sq2":
            squares()
        elif step[:4] == "pack":
            pack(int(step[4]))
        elif step[:6] == "routed":
            routed(int(step[6]))
        else:
            down(int(step[4]))
            give(int(step[4]))
    ret[pl.ds(0, SLOT)] = back[pl.ds(0, SLOT)]

    halo_up.wait_send()
    halo_down.wait_send()
    for g in gathers:
        g.drain()

    def drain_sp(k, c):
        carry_copy(k).wait_send()
        go(k, k, 1).wait_send()
        re(k, k, 1).wait_send()
        return c

    def drain_tp(k, c):
        for buf, send, recv in ((sqb, sq_s, sq_r), (sq2b, sq2_s, sq2_r)):
            pltpu.make_async_remote_copy(
                src_ref=buf.at[t],
                dst_ref=buf.at[t],
                send_sem=send.at[k],
                recv_sem=recv.at[t],
                device_id={"tp": lax.rem(t + k, NTP)},
                device_id_type=MESH,
            ).wait_send()
        return c

    weights = rw_ref[...]
    w0 = jnp.transpose(jnp.broadcast_to(weights[0:1], (128, TOK)))
    w1 = jnp.transpose(jnp.broadcast_to(weights[1:2], (128, TOK)))
    lax.fori_loop(1, NTP, drain_tp, 0)
    half = ROWS // 2

    def combine(c):
        at = pl.ds(c * half, half)
        got = ret[at]
        return w0 * dot(pk0[:, at], got) + w1 * dot(pk1[:, at], got)

    arrived(re, 16, NSP)
    resid[...] += combine(1)
    arrived(re, 1, 16)
    out_ref[...] = (resid[...] + combine(0)).astype(BF)
    lax.fori_loop(1, NSP, drain_sp, 0)


def layer(
    rec_input,
    gate_input,
    conv_weight,
    decay_wide,
    decay_narrow,
    input_wide,
    input_narrow,
    decay_base,
    decay_extra,
    tokens,
    out_weight,
    norm_gain,
    shared_gate,
    shared_up,
    shared_down,
    expert_gate,
    expert_up,
    expert_down,
    routes,
    route_weight,
):
    vmem = pl.BlockSpec(memory_space=pltpu.VMEM)
    hbm = pl.BlockSpec(memory_space=pl.ANY)
    dma = pltpu.SemaphoreType.DMA
    gather_sems = [dma((2, 20)), dma((2, len(RECV)))] * 11
    return pl.pallas_call(
        kernel,
        out_shape=jax.ShapeDtypeStruct((TOK, 128), BF),
        in_specs=[vmem] * 10 + [hbm] + [vmem] + [hbm] * 6 + [vmem] * 2,
        out_specs=vmem,
        scratch_shapes=[
            pltpu.VMEM((TOK + 24, CH), F32),
            pltpu.VMEM((16, CH), F32),
            pltpu.VMEM((8, CH), F32),
            pltpu.VMEM((2, TOK, CH), F32),
            pltpu.VMEM((2, TOK, CH), F32),
            pltpu.VMEM((TOK, CH), F32),
            pltpu.VMEM((2, 2, CH), F32),
            pltpu.VMEM((NSP, 2, CH), F32),
            pltpu.VMEM((NTP, 2 * MIXR, 128), BF),
            pltpu.VMEM((NTP, WIDE, 128), BF),
            pltpu.VMEM((NTP, WIDE, 256), BF),
            pltpu.VMEM((D, 256), BF),
            pltpu.VMEM((D, 256), BF),
            pltpu.VMEM((D, 128), BF),
            pltpu.VMEM((D, 128), BF),
            pltpu.VMEM((TOK, 128), F32),
            pltpu.VMEM((NTP, 1, TOK), F32),
            pltpu.VMEM((NTP, 1, DENSE), F32),
            pltpu.VMEM((DENSE, 128), F32),
            pltpu.VMEM((NTP, TOK, 128), BF),
            pltpu.VMEM((NTP, TOK, 128), BF),
            pltpu.VMEM((NTP, DENSE, 128), BF),
            pltpu.VMEM((NTP, DENSE, 128), BF),
            pltpu.VMEM((ROWS, 128), BF),
            pltpu.VMEM((ROWS, 128), BF),
            pltpu.VMEM((ROWS, 128), BF),
            pltpu.VMEM((ROWS, 128), BF),
            pltpu.VMEM((ROWS, TOK), BF),
            pltpu.VMEM((TOK, ROWS), BF),
            pltpu.VMEM((TOK, ROWS), BF),
            dma((9,)),
            dma((2,)),
            dma((2,)),
            dma((NSP,)),
            dma((NSP,)),
            dma((NTP,)),
            dma((NTP,)),
            dma((NTP,)),
            dma((NTP,)),
            dma((NSP,)),
            dma((NSP,)),
            dma((NSP,)),
            dma((NSP,)),
            *gather_sems,
        ],
        compiler_params=pltpu.CompilerParams(
            collective_id=0, has_side_effects=True, vmem_limit_bytes=60 * 1024 * 1024
        ),
        name="layer",
    )(
        rec_input.T,
        gate_input.T,
        conv_weight,
        decay_wide[:, 0],
        decay_narrow[:, 0],
        input_wide[:, 0],
        input_narrow[:, 0],
        decay_base,
        decay_extra.transpose(0, 2, 3, 1),
        tokens,
        out_weight.reshape(NTP, CH, 128),
        norm_gain.reshape(1, 128),
        shared_gate,
        shared_up,
        shared_down,
        expert_gate[0],
        expert_up[0],
        expert_down[0],
        routes.T,
        route_weight.T,
    )


def solution(mesh):
    return jax.shard_map(
        layer,
        mesh=mesh,
        in_specs=(
            P("sp", "tp"),
            P("sp", "tp"),
            P(None, "tp"),
            P(None, "tp", None, None),
            P(None, "tp", None, None),
            P(None, "tp", None, None),
            P(None, "tp", None, None),
            P(None, "tp"),
            P(None, "sp", None, "tp"),
            P("sp", "tp"),
            P(None, "tp"),
            P("tp"),
            P(None, "tp"),
            P(None, "tp"),
            P(None, "tp"),
            P("sp", None, "tp"),
            P("sp", None, "tp"),
            P("sp", None, "tp"),
            P("sp", None),
            P("sp", None),
        ),
        out_specs=P("sp", "tp"),
        check_vma=False,
    )
```

```python
import functools

import jax
import jax.numpy as jnp
from jax import lax
from jax.experimental import pallas as pl
from jax.experimental.pallas import tpu as pltpu
from jax.sharding import PartitionSpec as P

MESH = pl.DeviceIdType.MESH
BF = jnp.bfloat16
F32 = jnp.float32
D = 2048
NORM_EPS = 1e-06
RATE_SCALE = 8.0
NSP = 32
NTP = 16
TOK = 384
CH = 192
WIDE = 128
STEPS = 48
SLOT = 40
ROWS = NSP * SLOT
PAIR = 72
DENSE = NSP * 36
FAR = DENSE // 2
CHUNK = DENSE // 4
MIXR = 576


def iota(shape, dim):
    return lax.broadcasted_iota(jnp.int32, shape, dim)


def dot(a, b, ca=1, cb=0):
    return lax.dot_general(a, b, (((ca,), (cb,)), ((), ())), preferred_element_type=F32)


def neg_expm1(u):
    poly = u / 40320.0 + 1.0 / 5040.0
    for c in (720.0, 120.0, 24.0, 6.0, 2.0, 1.0):
        poly = poly * u + 1.0 / c
    return -jnp.where(u > -0.5, poly * u, jnp.exp(u) - 1.0)


def silu(x):
    return x * jax.nn.sigmoid(x)


MIX_ORDER = (
    (0, 0, 0, 1, 0), (0, 0, 0, 3, 0), (0, 0, 1, 0, 0), (0, 0, 3, 0, 0), (0, 1, 0, 1, 0),
    (0, 1, 0, 3, 0), (0, 1, 1, 0, 0), (0, 1, 3, 0, 0), (0, 0, 2, 0, 0), (0, 0, 2, 0, 1),
    (0, 0, 1, 1, 0), (0, 0, 1, 3, 0), (0, 0, 3, 1, 0), (0, 1, 1, 1, 0), (0, 0, 3, 3, 0),
    (0, 1, 1, 3, 0), (0, 1, 2, 0, 0), (0, 1, 2, 0, 1), (0, 1, 3, 1, 0), (0, 1, 3, 3, 0),
    (0, 0, 2, 1, 0), (0, 0, 2, 3, 0), (0, 1, 2, 1, 0), (0, 1, 2, 3, 0),
)
ORDER = (
    (0, 0, 0, 1, 0), (0, 0, 0, 3, 0), (0, 0, 1, 0, 0), (0, 0, 3, 0, 0), (0, 1, 0, 1, 0),
    (0, 1, 0, 3, 0), (0, 1, 1, 0, 0), (0, 1, 3, 0, 0), (0, 0, 2, 0, 0), (0, 0, 2, 0, 1),
    (0, 0, 1, 1, 0), (0, 0, 1, 3, 0), (0, 0, 3, 1, 0), (0, 1, 1, 1, 0), (0, 0, 3, 3, 0),
    (0, 1, 1, 3, 0), (0, 1, 2, 0, 0), (0, 1, 2, 0, 1), (0, 1, 3, 1, 0), (0, 1, 3, 3, 0),
    (0, 0, 2, 1, 0), (0, 0, 2, 3, 0), (0, 1, 2, 1, 0), (0, 1, 2, 3, 0), "shared", "pack3",
    (1, 0, 0, 1, 0), (1, 0, 0, 3, 0), (1, 0, 1, 0, 0), (1, 0, 3, 0, 0), (1, 1, 0, 1, 0),
    (1, 1, 0, 3, 0), (1, 1, 1, 0, 0), (1, 1, 3, 0, 0), "pack2", (5, 0, 0, 1, 0), (5, 0, 0, 3, 0),
    (5, 0, 1, 0, 0), (5, 0, 3, 0, 0), (5, 1, 0, 1, 0), (5, 1, 0, 3, 0), (5, 1, 1, 0, 0),
    (5, 1, 3, 0, 0), (1, 0, 2, 0, 0), (1, 0, 2, 0, 1), (1, 0, 1, 1, 0), (1, 0, 1, 3, 0),
    (1, 0, 3, 1, 0), (1, 1, 1, 1, 0), (1, 0, 3, 3, 0), (1, 1, 1, 3, 0), (1, 1, 2, 0, 0),
    (1, 1, 2, 0, 1), (1, 1, 3, 1, 0), (1, 1, 3, 3, 0), (4, 0, 0, 1, 0), (4, 0, 0, 3, 0),
    (4, 0, 1, 0, 0), (4, 0, 3, 0, 0), (4, 1, 1, 0, 0), (4, 1, 3, 0, 0), (4, 1, 0, 1, 0),
    (4, 1, 0, 3, 0), (5, 0, 2, 0, 0), (5, 0, 2, 0, 1), (5, 0, 1, 1, 0), (5, 0, 1, 3, 0),
    (5, 0, 3, 1, 0), (5, 0, 3, 3, 0), (5, 1, 1, 1, 0), (5, 1, 1, 3, 0), "pack1", (5, 1, 2, 0, 0),
    (5, 1, 2, 0, 1), (5, 1, 3, 1, 0), (5, 1, 3, 3, 0), (1, 0, 2, 1, 0), (1, 0, 2, 3, 0),
    (1, 1, 2, 1, 0), (1, 1, 2, 3, 0), (4, 0, 2, 0, 0), (4, 0, 2, 0, 1), (4, 0, 1, 1, 0),
    (4, 0, 1, 3, 0), (4, 1, 1, 1, 0), (4, 1, 1, 3, 0), (4, 0, 3, 1, 0), (4, 0, 3, 3, 0),
    (4, 1, 2, 0, 0), (4, 1, 2, 0, 1), (4, 1, 3, 1, 0), (4, 1, 3, 3, 0), "pack0", "sq2",
    (5, 0, 2, 1, 0), (5, 0, 2, 3, 0), (3, 0, 1, 0, 0), (3, 0, 3, 0, 0), (3, 0, 0, 1, 0),
    (3, 0, 0, 3, 0), (3, 1, 0, 1, 0), (3, 1, 0, 3, 0), (3, 1, 1, 0, 0), (3, 1, 3, 0, 0),
    (5, 1, 2, 1, 0), (5, 1, 2, 3, 0), "sdown", (4, 0, 2, 1, 0), (4, 0, 2, 3, 0), (4, 1, 2, 1, 0),
    (4, 1, 2, 3, 0), (2, 0, 0, 1, 0), (2, 0, 0, 3, 0), (2, 0, 1, 0, 0), (2, 0, 3, 0, 0),
    (2, 1, 1, 0, 0), (2, 1, 3, 0, 0), (2, 1, 0, 1, 0), (2, 1, 0, 3, 0), (3, 0, 2, 0, 0),
    (3, 0, 2, 0, 1), (3, 0, 1, 1, 0), (3, 0, 1, 3, 0), (3, 0, 3, 1, 0), (3, 0, 3, 3, 0),
    (3, 1, 1, 1, 0), (3, 1, 1, 3, 0), (3, 1, 2, 0, 0), (3, 1, 2, 0, 1), (3, 1, 3, 1, 0),
    (3, 1, 3, 3, 0), "routed3", (2, 0, 2, 0, 0), (2, 0, 2, 0, 1), (2, 0, 1, 1, 0), (2, 0, 1, 3, 0),
    "routed2", (2, 1, 1, 1, 0), (2, 1, 1, 3, 0), (2, 0, 3, 1, 0), (2, 0, 3, 3, 0), (2, 1, 2, 0, 0),
    (2, 1, 2, 0, 1), (2, 1, 3, 1, 0), (2, 1, 3, 3, 0), (3, 0, 2, 1, 0), (3, 0, 2, 3, 0),
    (3, 1, 2, 1, 0), (3, 1, 2, 3, 0), (9, 0, 0, 1, 0), (9, 0, 0, 3, 0), (9, 0, 1, 0, 0),
    (9, 0, 3, 0, 0), (9, 1, 1, 0, 0), (9, 1, 3, 0, 0), (9, 1, 0, 1, 0), (9, 1, 0, 3, 0),
    (2, 0, 2, 1, 0), (2, 0, 2, 3, 0), (8, 0, 1, 0, 0), (8, 0, 3, 0, 0), (8, 0, 0, 1, 0),
    (8, 0, 0, 3, 0), (8, 1, 0, 1, 0), (8, 1, 0, 3, 0), (8, 1, 1, 0, 0), (8, 1, 3, 0, 0),
    (2, 1, 2, 1, 0), (2, 1, 2, 3, 0), "routed1", (9, 0, 2, 0, 0), (9, 0, 2, 0, 1), (9, 0, 1, 1, 0),
    (9, 0, 1, 3, 0), (9, 1, 1, 1, 0), (9, 1, 1, 3, 0), (9, 0, 3, 1, 0), (9, 0, 3, 3, 0),
    (9, 1, 2, 0, 0), (9, 1, 2, 0, 1), (9, 1, 3, 1, 0), (9, 1, 3, 3, 0), (8, 0, 2, 0, 0),
    (8, 0, 2, 0, 1), (8, 0, 1, 1, 0), (8, 0, 1, 3, 0), (8, 0, 3, 1, 0), (8, 0, 3, 3, 0),
    (8, 1, 1, 1, 0), (8, 1, 1, 3, 0), (8, 1, 2, 0, 0), (8, 1, 2, 0, 1), (8, 1, 3, 1, 0),
    (8, 1, 3, 3, 0), "routed0", (7, 0, 0, 1, 0), (7, 0, 0, 3, 0), (7, 0, 1, 0, 0), (7, 0, 3, 0, 0),
    (7, 1, 1, 0, 0), (7, 1, 3, 0, 0), (7, 1, 0, 1, 0), (7, 1, 0, 3, 0), (9, 0, 2, 1, 0),
    (9, 0, 2, 3, 0), (9, 1, 2, 1, 0), (9, 1, 2, 3, 0), (8, 0, 2, 1, 0), (8, 0, 2, 3, 0),
    (8, 1, 2, 1, 0), (8, 1, 2, 3, 0), (6, 0, 0, 1, 0), (6, 0, 0, 3, 0), (6, 0, 1, 0, 0),
    (6, 0, 3, 0, 0), (6, 1, 1, 0, 0), (6, 1, 3, 0, 0), (6, 1, 0, 1, 0), (6, 1, 0, 3, 0),
    (7, 0, 2, 0, 0), (7, 0, 2, 0, 1), (7, 0, 1, 1, 0), (7, 0, 1, 3, 0), (7, 1, 1, 1, 0),
    (7, 1, 1, 3, 0), (7, 0, 3, 1, 0), (7, 0, 3, 3, 0), (7, 1, 2, 0, 0), (7, 1, 2, 0, 1),
    (7, 1, 3, 1, 0), (7, 1, 3, 3, 0), "down3", (6, 0, 2, 0, 0), (6, 0, 2, 0, 1), "down2",
    (6, 0, 1, 1, 0), (6, 0, 1, 3, 0), (6, 1, 1, 1, 0), (6, 1, 1, 3, 0), (6, 0, 3, 1, 0),
    (6, 0, 3, 3, 0), (6, 1, 2, 0, 0), (6, 1, 2, 0, 1), (6, 1, 3, 1, 0), (6, 1, 3, 3, 0),
    (7, 0, 2, 1, 0), (7, 0, 2, 3, 0), (7, 1, 2, 1, 0), (7, 1, 2, 3, 0), (6, 0, 2, 1, 0),
    (6, 0, 2, 3, 0), (6, 1, 2, 1, 0), (6, 1, 2, 3, 0), "down1", "down0",
)


RECV = {}
for _da in range(4):
    for _db in range(4):
        if (_da, _db) != (0, 0):
            for _q in range(2 if _db == 2 or (_da, _db) == (2, 0) else 1):
                RECV[_da, _db, _q] = len(RECV)


class Gather:
    def __init__(self, buf, base, rows, send, recv):
        self.buf, self.base, self.rows, self.send, self.recv = buf, base, rows, send, recv
        t = lax.axis_index("tp")
        self.x, self.y = lax.rem(t, 4), lax.div(t, 4)
        self.sent = []
        self.count = [0, 0]
        self.seen = [0, 0]

    def where(self, h, da, db):
        a, b = (self.x, self.y) if h == 0 else (self.y, self.x)
        a, b = lax.rem(a + (da + 8), 4), lax.rem(b + (db + 8), 4)
        return b * 4 + a if h == 0 else a * 4 + b

    def part(self, h, q):
        half, quarter = self.rows // 2, self.rows // 4
        if q is None:
            return pl.ds(self.base + h * half, half)
        return pl.ds(self.base + h * half + q * quarter, quarter)

    def put(self, h, da, db, q, ta, tb):
        at = self.buf.at[self.where(h, -da, -db), self.part(h, q)]
        c = pltpu.make_async_remote_copy(
            src_ref=at,
            dst_ref=at,
            send_sem=self.send.at[h, self.count[h]],
            recv_sem=self.recv.at[h, RECV[(da + ta) % 4, (db + tb) % 4, q or 0]],
            device_id={"tp": self.where(h, ta, tb)},
            device_id_type=MESH,
        )
        self.count[h] += 1
        c.start()
        self.sent.append(c)

    def wait(self, h, da, db, q):
        split = db == 2 or (da, db) == (2, 0)
        at = self.buf.at[self.where(h, -da, -db), self.part(h, q if split else None)]
        pltpu.make_async_remote_copy(
            src_ref=at,
            dst_ref=at,
            send_sem=self.send.at[h, 0],
            recv_sem=self.recv.at[h, RECV[da, db, q or 0]],
            device_id={"tp": self.where(h, 1, 0)},
            device_id_type=MESH,
        ).wait_recv()

    def start(self):
        for h in range(2):
            for ta, tb in ((1, 0), (-1, 0), (0, 1), (0, -1)):
                self.put(h, 0, 0, None, ta, tb)

    def take(self, h, da, db, q):
        self.wait(h, da, db, q)
        if db == 0 and da != 2:
            self.put(h, da, 0, 0 if da == 1 else 1, 2 - da, 0)
        if db == 0:
            self.seen[h] += da == 2
            if da != 2 or self.seen[h] == 2:
                self.put(h, da, 0, None, 0, 1)
                self.put(h, da, 0, None, 0, -1)
        else:
            self.put(h, da, db, 0 if db == 1 else 1, 0, 2 - db)

    def finish(self):
        for da in (0, 1, 3, 2):
            for h in range(2):
                for q in range(2):
                    self.wait(h, da, 2, q)

    def drain(self):
        for c in self.sent:
            c.wait_send()


def kernel(
    rec_ref,
    gate_ref,
    conv_ref,
    dw_ref,
    dn_ref,
    iw_ref,
    in_ref,
    base_ref,
    extra_ref,
    tok_ref,
    outw_ref,
    gain_ref,
    sg_ref,
    su_ref,
    sd_ref,
    eg_ref,
    eu_ref,
    ed_ref,
    routes_ref,
    rw_ref,
    out_ref,
    rp,
    hl,
    hr,
    av,
    bv,
    gp,
    tot,
    car,
    mixb,
    wd,
    ww,
    wsgu,
    wegu,
    wsd,
    wed,
    resid,
    sqb,
    sq2b,
    sc2,
    nbuf,
    hsbuf,
    rbuf,
    hrbuf,
    outgo,
    arr,
    back,
    ret,
    pt,
    pk0,
    pk1,
    wsem,
    halo_s,
    halo_r,
    car_s,
    car_r,
    sq_s,
    sq_r,
    sq2_s,
    sq2_r,
    go_s,
    go_r,
    re_s,
    re_r,
    *gather_sems,
):
    s, t = lax.axis_index("sp"), lax.axis_index("tp")

    barrier = pltpu.get_barrier_semaphore()

    def greet_sp(k, c):
        pl.semaphore_signal(
            barrier, inc=1, device_id={"sp": lax.rem(s + k, NSP)}, device_id_type=MESH
        )
        return c

    def greet_tp(k, c):
        pl.semaphore_signal(
            barrier, inc=1, device_id={"tp": lax.rem(t + k, NTP)}, device_id_type=MESH
        )
        return c

    lax.fori_loop(1, NSP, greet_sp, 0)
    lax.fori_loop(1, NTP, greet_tp, 0)

    r_i, t_i = iota((TOK, TOK), 0), iota((TOK, TOK), 1)
    order = (t_i == (r_i & 7) * STEPS + (r_i >> 3)).astype(BF)
    rp[pl.ds(16, TOK)] = dot(order, rec_ref[...], 1, 1)

    pl.semaphore_wait(barrier, NSP - 1 + NTP - 1)

    up, down = lax.rem(s + 1, NSP), lax.rem(s + NSP - 1, NSP)
    halo_up = pltpu.make_async_remote_copy(
        src_ref=rp.at[pl.ds(16 + 46 * 8, 16)],
        dst_ref=hl,
        send_sem=halo_s.at[0],
        recv_sem=halo_r.at[0],
        device_id={"sp": up},
        device_id_type=MESH,
    )
    halo_up.start()
    halo_down = pltpu.make_async_remote_copy(
        src_ref=rp.at[pl.ds(16, 8)],
        dst_ref=hr,
        send_sem=halo_s.at[1],
        recv_sem=halo_r.at[1],
        device_id={"sp": down},
        device_id_type=MESH,
    )
    halo_down.start()

    loads = []

    def load(src, dst):
        c = pltpu.make_async_copy(src, dst, wsem.at[len(loads)])
        c.start()
        loads.append(c)

    ww[...] = jnp.zeros_like(ww)
    load(outw_ref.at[:, pl.ds(0, WIDE)], wd)
    load(outw_ref.at[:, pl.ds(WIDE, 64)], ww.at[:, pl.ds(0, 64), pl.ds(0, 128)])
    load(outw_ref.at[:, pl.ds(WIDE, 64)], ww.at[:, pl.ds(64, 64), pl.ds(128, 128)])
    n_out = len(loads)
    load(sg_ref, wsgu.at[:, pl.ds(0, 128)])
    load(su_ref, wsgu.at[:, pl.ds(128, 128)])
    load(sd_ref, wsd)
    n_shared = len(loads)
    load(eg_ref, wegu.at[:, pl.ds(0, 128)])
    load(eu_ref, wegu.at[:, pl.ds(128, 128)])
    load(ed_ref, wed)


    for d in range(2):
        rows = jnp.concatenate(
            [
                jnp.broadcast_to(extra_ref[d, 0], (WIDE, TOK)),
                jnp.broadcast_to(extra_ref[d, 1], (CH - WIDE, TOK)),
            ],
            axis=0,
        )
        high = rows.astype(BF)
        left = rows - high.astype(F32)
        mid = left.astype(BF)
        low = (left - mid.astype(F32)).astype(BF)
        av[d] = (dot(order, high, 1, 1) + dot(order, mid, 1, 1)) + dot(order, low, 1, 1)

    taps = conv_ref[...].astype(F32)

    block = 64

    def gates(i):
        r0 = i * block
        conv = rp[pl.ds(r0, block)] * taps[0:1]
        for j in range(1, 4):
            conv = conv + rp[pl.ds(r0 + 8 * j, block)] * taps[j : j + 1]
        conv_b = conv.astype(BF)
        conv_f = conv_b.astype(F32)
        wide, narrow = conv_b[:, :WIDE], conv_b[:, WIDE:]
        for d in range(2):
            rate = jax.nn.sigmoid(
                jnp.concatenate([dot(wide, dw_ref[d]), dot(narrow, dn_ref[d])], axis=1)
            )
            admit = jax.nn.sigmoid(
                jnp.concatenate([dot(wide, iw_ref[d]), dot(narrow, in_ref[d])], axis=1)
            )
            log_decay = -RATE_SCALE * rate * base_ref[d : d + 1] + av[d, pl.ds(r0, block)]
            drive = jnp.sqrt(neg_expm1(2.0 * log_decay)) * admit * conv_f
            av[d, pl.ds(r0, block)] = jnp.exp(log_decay)
            bv[d, pl.ds(r0, block)] = drive

    for i in range(1, 5):
        gates(i)
    halo_up.wait_recv()
    halo_down.wait_recv()
    sub = iota((8, CH), 0)
    first, last = s == 0, s == NSP - 1
    for k in range(2):
        edge = jnp.where(first, 0.0, hl[pl.ds(k * 8 + 7, 1)])
        rolled = pltpu.roll(rp[pl.ds(16 + (46 + k) * 8, 8)], 1, 0)
        rp[pl.ds(k * 8, 8)] = jnp.where(sub == 0, edge, rolled)
    edge = jnp.where(last, 0.0, hr[pl.ds(0, 1)])
    rolled = pltpu.roll(rp[pl.ds(16, 8)], 7, 0)
    rp[pl.ds(16 + TOK, 8)] = jnp.where(sub == 7, edge, rolled)
    gates(0)
    gates(5)

    def scan(i, carry):
        c0, s0, c1, s1 = carry
        f = pl.ds(pl.multiple_of(i * 8, 8), 8)
        g = pl.ds(pl.multiple_of((STEPS - 1 - i) * 8, 8), 8)
        a0, a1 = av[0, f], av[1, g]
        s0, s1 = a0 * s0 + bv[0, f], a1 * s1 + bv[1, g]
        c0, c1 = a0 * c0, a1 * c1
        av[0, f], av[1, g] = c0, c1
        bv[0, f], bv[1, g] = s0, s1
        return c0, s0, c1, s1

    one, zero = jnp.ones((8, CH), F32), jnp.zeros((8, CH), F32)
    c0, s0, c1, s1 = lax.fori_loop(0, STEPS, scan, (one, zero, one, zero), unroll=4)

    def chunks(c, st, sequence):
        g, h = jnp.ones((1, CH), F32), jnp.zeros((1, CH), F32)
        gin, hin = zero, zero
        for k in sequence:
            gin = jnp.where(sub == k, g, gin)
            hin = jnp.where(sub == k, h, hin)
            ck, sk = c[k : k + 1], st[k : k + 1]
            g, h = ck * g, ck * h + sk
        return gin, hin, g, h

    g0, h0, gt0, ht0 = chunks(c0, s0, range(8))
    g1, h1, gt1, ht1 = chunks(c1, s1, range(7, -1, -1))
    tot[0, pl.ds(0, 1)] = gt0
    tot[0, pl.ds(1, 1)] = ht0
    tot[1, pl.ds(0, 1)] = gt1
    tot[1, pl.ds(1, 1)] = ht1

    def carry_copy(k):
        dest = lax.rem(s + k, NSP)
        return pltpu.make_async_remote_copy(
            src_ref=tot.at[(dest < s).astype(jnp.int32)],
            dst_ref=car.at[s],
            send_sem=car_s.at[k],
            recv_sem=car_r.at[s],
            device_id={"sp": dest},
            device_id_type=MESH,
        )

    def carry_start(k, c):
        carry_copy(k).start()
        return c

    lax.fori_loop(1, NSP, carry_start, 0)
    car[s] = jnp.zeros((2, CH), F32)

    gp[...] = jax.nn.gelu(dot(order, gate_ref[...], 1, 1))
    routes = routes_ref[...].astype(F32)
    e0, e1 = routes[0:1], routes[1:2]
    e_i = iota((NSP, TOK), 0).astype(F32)
    hit0, hit1 = e_i == e0, e_i == e1
    named = jnp.where(hit0, 1.0, 0.0) + jnp.where(hit1, 1.0, 0.0)
    rank = dot(named.astype(BF), (r_i < t_i).astype(BF))
    def rel(e):
        k = e - s.astype(F32)
        k = jnp.where(k < 0.0, k + NSP, k)
        return jnp.where(k > 16.0, 64.0 - 2.0 * k, jnp.maximum(2.0 * k - 1.0, 0.0))

    place0 = rel(e0) * SLOT + jnp.sum(jnp.where(hit0, rank, 0.0), axis=0, keepdims=True)
    place1 = rel(e1) * SLOT + jnp.sum(jnp.where(hit1, rank, 0.0), axis=0, keepdims=True)
    for k in range(ROWS // 128):
        s_i = (iota((128, TOK), 0) + k * 128).astype(F32)
        pt[pl.ds(k * 128, 128)] = (
            jnp.where(s_i == place0, 1.0, 0.0) + jnp.where(s_i == place1, 1.0, 0.0)
        ).astype(BF)
    col0 = jnp.transpose(jnp.broadcast_to(place0, (128, TOK)))
    col1 = jnp.transpose(jnp.broadcast_to(place1, (128, TOK)))
    for k in range(ROWS // 128):
        l_i = (iota((TOK, 128), 1) + k * 128).astype(F32)
        pk0[:, pl.ds(k * 128, 128)] = jnp.where(l_i == col0, 1.0, 0.0).astype(BF)
        pk1[:, pl.ds(k * 128, 128)] = jnp.where(l_i == col1, 1.0, 0.0).astype(BF)


    def carry_wait(k, c):
        src = lax.rem(s + k, NSP)
        pltpu.make_async_remote_copy(
            src_ref=tot.at[0],
            dst_ref=car.at[src],
            send_sem=car_s.at[k],
            recv_sem=car_r.at[src],
            device_id={"sp": src},
            device_id_type=MESH,
        ).wait_recv()
        return c

    lax.fori_loop(1, NSP, carry_wait, 0)
    ahead, behind = jnp.zeros((1, CH), F32), jnp.zeros((1, CH), F32)
    for j in range(NSP):
        cj = car[j]
        ahead = jnp.where(j < s, cj[0:1] * ahead + cj[1:2], ahead)
        cj = car[NSP - 1 - j]
        behind = jnp.where(NSP - 1 - j > s, cj[0:1] * behind + cj[1:2], behind)
    x0, x1 = h0 + g0 * ahead, h1 + g1 * behind

    for i in range(STEPS):
        f = pl.ds(i * 8, 8)
        total = (bv[0, f] + av[0, f] * x0) + (bv[1, f] + av[1, f] * x1)
        bv[0, f] = total * gp[f]
    tok_i, row_i = iota((TOK, TOK), 0), iota((TOK, TOK), 1)
    chunk = sum(jnp.where(tok_i >= STEPS * k, 1, 0) for k in range(1, 8))
    back_order = (row_i == (tok_i - chunk * STEPS) * 8 + chunk).astype(BF)
    mixed = dot(back_order, bv[0].astype(BF)).astype(BF)
    c_i, l_i = iota((CH, 128), 0), iota((CH, 128), 1)
    low = ((c_i == l_i + WIDE) & (l_i < 64)).astype(BF)
    high = ((c_i == l_i + 64) & (l_i >= 64)).astype(BF)
    gathers = [
        Gather(buf, base, rows, *gather_sems[2 * k : 2 * k + 2])
        for k, (buf, base, rows) in enumerate(
            (
                (mixb, 0, MIXR),
                (nbuf, 0, TOK),
                (hsbuf, 0, TOK),
                *((b, c * CHUNK, CHUNK) for b in (rbuf, hrbuf) for c in range(4)),
            )
        )
    ]
    gm, gn, gs = gathers[:3]
    gr, gf = gathers[3:7], gathers[7:]
    mixb[t, pl.ds(0, TOK)] = mixed[:, :WIDE]
    mixb[t, pl.ds(TOK, 192)] = (dot(mixed[:192], low) + dot(mixed[192:], high)).astype(BF)
    gm.start()
    for _, *way in MIX_ORDER:
        gm.take(*way)
    gm.finish()
    for c in loads[:n_out]:
        c.wait()

    lhs = jnp.concatenate([mixb[j, pl.ds(0, TOK)] for j in range(NTP)], axis=1)
    res = tok_ref[...].astype(F32) + dot(lhs, wd[...].reshape(NTP * WIDE, 128))
    lhs = jnp.concatenate([mixb[j, pl.ds(TOK, 192)] for j in range(NTP)], axis=1)
    add = dot(lhs, ww[...].reshape(NTP * WIDE, 256))
    res = res + jnp.concatenate([add[:, :128], add[:, 128:]], axis=0)
    resid[...] = res
    nbuf[t] = (res * gain_ref[...]).astype(BF)
    gn.start()

    outgo[...] = dot(pt[...], nbuf[t]).astype(BF)

    def place(p):
        return pl.ds(pl.multiple_of(p * SLOT, 8), SLOT)

    def both_ways(a, b, op):
        def step(m, c):
            op(2 * m - 1, 2 * m, m)
            op(2 * m, 2 * m - 1, -m)
            return c

        lax.fori_loop(a, b, step, 0)

    def exchange(src, dst, send, recv):
        def copy(p, q, k):
            return pltpu.make_async_remote_copy(
                src_ref=src.at[place(p)],
                dst_ref=dst.at[place(q)],
                send_sem=send.at[p],
                recv_sem=recv.at[q],
                device_id={"sp": lax.rem(s + k + NSP, NSP)},
                device_id_type=MESH,
            )

        return copy

    go, re = exchange(outgo, arr, go_s, go_r), exchange(back, ret, re_s, re_r)
    go(31, 31, 16).start()

    def go_start(i, c):
        m = 16 - i
        go(2 * m, 2 * m - 1, -m).start()
        go(2 * m - 1, 2 * m, m).start()
        return c

    lax.fori_loop(1, 16, go_start, 0)
    arr[pl.ds(0, SLOT)] = outgo[pl.ds(0, SLOT)]

    def arrived(copy, a, b):
        def step(p, c):
            copy(p, p, 1).wait_recv()
            return c

        lax.fori_loop(a, b, step, 0)

    def spread_sums(buf, send, recv):
        def step(k, c):
            pltpu.make_async_remote_copy(
                src_ref=buf.at[t],
                dst_ref=buf.at[t],
                send_sem=send.at[k],
                recv_sem=recv.at[t],
                device_id={"tp": lax.rem(t + k, NTP)},
                device_id_type=MESH,
            ).start()
            return c

        lax.fori_loop(1, NTP, step, 0)

    def total_scale(buf, send, recv):
        def step(k, c):
            src = lax.rem(t + k, NTP)
            pltpu.make_async_remote_copy(
                src_ref=buf.at[t],
                dst_ref=buf.at[src],
                send_sem=send.at[k],
                recv_sem=recv.at[src],
                device_id={"tp": src},
                device_id_type=MESH,
            ).wait_recv()
            return c

        lax.fori_loop(1, NTP, step, 0)
        square = buf[0]
        for j in range(1, NTP):
            square = square + buf[j]
        root = lax.rsqrt(square / D + NORM_EPS)
        return jnp.transpose(jnp.broadcast_to(root, (128, root.shape[1])))

    sqb[t] = jnp.sum(jnp.transpose(res * res), axis=0, keepdims=True)
    spread_sums(sqb, sq_s, sq_r)

    p_i, q_i = iota((PAIR, 2 * SLOT), 0), iota((PAIR, 2 * SLOT), 1)
    squeeze = (q_i == p_i + jnp.where(p_i >= 36, SLOT - 36, 0)).astype(BF)
    p_i, q_i = iota((2 * SLOT, PAIR), 0), iota((2 * SLOT, PAIR), 1)
    spread = (p_i == q_i + jnp.where(q_i >= 36, SLOT - 36, 0)).astype(BF)

    def pack(c):
        arrived(go, max(c * 8, 1), c * 8 + 8)
        for k in range(4):
            rows = arr[pl.ds((c * 4 + k) * 2 * SLOT, 2 * SLOT)]
            rbuf[t, pl.ds((c * 4 + k) * PAIR, PAIR)] = dot(squeeze, rows).astype(BF)
        gr[c].start()

    def squares():
        mine = rbuf[t].astype(F32) * (1.0 / gain_ref[...])
        sq2b[t] = jnp.sum(jnp.transpose(mine * mine), axis=0, keepdims=True)
        spread_sums(sq2b, sq2_s, sq2_r)

    def shared():
        gn.finish()
        scale = total_scale(sqb, sq_s, sq_r)
        for c in loads[n_out:n_shared]:
            c.wait()
        lhs = jnp.concatenate([nbuf[j] for j in range(NTP)], axis=1)
        both = dot(lhs, wsgu[...])
        hsbuf[t] = (silu(both[:, :128] * scale) * (both[:, 128:] * scale)).astype(BF)
        gs.start()

    scaled = []

    def routed(c):
        gr[c].finish()
        if not scaled:
            sc2[...] = total_scale(sq2b, sq2_s, sq2_r)
            for w in loads[n_shared:]:
                w.wait()
            scaled.append(c)

        def step(i, carry):
            r = pl.ds(pl.multiple_of(c * CHUNK + i * (CHUNK // 2), 8), CHUNK // 2)
            left = jnp.concatenate([rbuf[j, r] for j in range(NTP)], axis=1)
            both = dot(left, wegu[...])
            sc = sc2[r]
            hrbuf[t, r] = (silu(both[:, :128] * sc) * (both[:, 128:] * sc)).astype(BF)
            return carry

        lax.fori_loop(0, 2, step, 0)
        gf[c].start()

    def shared_down():
        gs.finish()
        lhs = jnp.concatenate([hsbuf[j] for j in range(NTP)], axis=1)
        resid[...] += dot(lhs, wsd[...])

    def down(c):
        gf[c].finish()
        left = jnp.concatenate([hrbuf[j, pl.ds(c * CHUNK, CHUNK)] for j in range(NTP)], axis=1)
        y = dot(left, wed[...]).astype(BF)
        for k in range(4):
            back[pl.ds((c * 4 + k) * 2 * SLOT, 2 * SLOT)] = dot(
                spread, y[k * PAIR : (k + 1) * PAIR]
            ).astype(BF)

    def give(c):
        if c == 3:
            re(31, 31, 16).start()
        else:
            re(8 * c + 7, 8 * c + 8, 4 * c + 4).start()
        both_ways(4 * c + 1, 4 * c + 4, lambda p, q, k: re(p, q, k).start())
        if c:
            re(8 * c, 8 * c - 1, -4 * c).start()

    for step in ORDER:
        if not isinstance(step, str):
            gathers[step[0] + 1].take(*step[1:])
        elif step == "shared":
            shared()
        elif step == "sdown":
            shared_down()
        elif step == "sq2":
            squares()
        elif step[:4] == "pack":
            pack(int(step[4]))
        elif step[:6] == "routed":
            routed(int(step[6]))
        else:
            down(int(step[4]))
            give(int(step[4]))
    ret[pl.ds(0, SLOT)] = back[pl.ds(0, SLOT)]

    halo_up.wait_send()
    halo_down.wait_send()
    for g in gathers:
        g.drain()

    def drain_sp(k, c):
        carry_copy(k).wait_send()
        go(k, k, 1).wait_send()
        re(k, k, 1).wait_send()
        return c

    def drain_tp(k, c):
        for buf, send, recv in ((sqb, sq_s, sq_r), (sq2b, sq2_s, sq2_r)):
            pltpu.make_async_remote_copy(
                src_ref=buf.at[t],
                dst_ref=buf.at[t],
                send_sem=send.at[k],
                recv_sem=recv.at[t],
                device_id={"tp": lax.rem(t + k, NTP)},
                device_id_type=MESH,
            ).wait_send()
        return c

    weights = rw_ref[...]
    w0 = jnp.transpose(jnp.broadcast_to(weights[0:1], (128, TOK)))
    w1 = jnp.transpose(jnp.broadcast_to(weights[1:2], (128, TOK)))
    lax.fori_loop(1, NTP, drain_tp, 0)
    half = ROWS // 2

    def combine(c):
        at = pl.ds(c * half, half)
        got = ret[at]
        return w0 * dot(pk0[:, at], got) + w1 * dot(pk1[:, at], got)

    arrived(re, 16, NSP)
    resid[...] += combine(1)
    arrived(re, 1, 16)
    out_ref[...] = (resid[...] + combine(0)).astype(BF)
    lax.fori_loop(1, NSP, drain_sp, 0)


def layer(
    rec_input,
    gate_input,
    conv_weight,
    decay_wide,
    decay_narrow,
    input_wide,
    input_narrow,
    decay_base,
    decay_extra,
    tokens,
    out_weight,
    norm_gain,
    shared_gate,
    shared_up,
    shared_down,
    expert_gate,
    expert_up,
    expert_down,
    routes,
    route_weight,
):
    vmem = pl.BlockSpec(memory_space=pltpu.VMEM)
    hbm = pl.BlockSpec(memory_space=pl.ANY)
    dma = pltpu.SemaphoreType.DMA
    gather_sems = [dma((2, 20)), dma((2, len(RECV)))] * 11
    return pl.pallas_call(
        kernel,
        out_shape=jax.ShapeDtypeStruct((TOK, 128), BF),
        in_specs=[vmem] * 10 + [hbm] + [vmem] + [hbm] * 6 + [vmem] * 2,
        out_specs=vmem,
        scratch_shapes=[
            pltpu.VMEM((TOK + 24, CH), F32),
            pltpu.VMEM((16, CH), F32),
            pltpu.VMEM((8, CH), F32),
            pltpu.VMEM((2, TOK, CH), F32),
            pltpu.VMEM((2, TOK, CH), F32),
            pltpu.VMEM((TOK, CH), F32),
            pltpu.VMEM((2, 2, CH), F32),
            pltpu.VMEM((NSP, 2, CH), F32),
            pltpu.VMEM((NTP, 2 * MIXR, 128), BF),
            pltpu.VMEM((NTP, WIDE, 128), BF),
            pltpu.VMEM((NTP, WIDE, 256), BF),
            pltpu.VMEM((D, 256), BF),
            pltpu.VMEM((D, 256), BF),
            pltpu.VMEM((D, 128), BF),
            pltpu.VMEM((D, 128), BF),
            pltpu.VMEM((TOK, 128), F32),
            pltpu.VMEM((NTP, 1, TOK), F32),
            pltpu.VMEM((NTP, 1, DENSE), F32),
            pltpu.VMEM((DENSE, 128), F32),
            pltpu.VMEM((NTP, TOK, 128), BF),
            pltpu.VMEM((NTP, TOK, 128), BF),
            pltpu.VMEM((NTP, DENSE, 128), BF),
            pltpu.VMEM((NTP, DENSE, 128), BF),
            pltpu.VMEM((ROWS, 128), BF),
            pltpu.VMEM((ROWS, 128), BF),
            pltpu.VMEM((ROWS, 128), BF),
            pltpu.VMEM((ROWS, 128), BF),
            pltpu.VMEM((ROWS, TOK), BF),
            pltpu.VMEM((TOK, ROWS), BF),
            pltpu.VMEM((TOK, ROWS), BF),
            dma((9,)),
            dma((2,)),
            dma((2,)),
            dma((NSP,)),
            dma((NSP,)),
            dma((NTP,)),
            dma((NTP,)),
            dma((NTP,)),
            dma((NTP,)),
            dma((NSP,)),
            dma((NSP,)),
            dma((NSP,)),
            dma((NSP,)),
            *gather_sems,
        ],
        compiler_params=pltpu.CompilerParams(
            collective_id=0, has_side_effects=True, vmem_limit_bytes=60 * 1024 * 1024
        ),
        name="layer",
    )(
        rec_input.T,
        gate_input.T,
        conv_weight,
        decay_wide[:, 0],
        decay_narrow[:, 0],
        input_wide[:, 0],
        input_narrow[:, 0],
        decay_base,
        decay_extra.transpose(0, 2, 3, 1),
        tokens,
        out_weight.reshape(NTP, CH, 128),
        norm_gain.reshape(1, 128),
        shared_gate,
        shared_up,
        shared_down,
        expert_gate[0],
        expert_up[0],
        expert_down[0],
        routes.T,
        route_weight.T,
    )


def solution(mesh):
    return jax.shard_map(
        layer,
        mesh=mesh,
        in_specs=(
            P("sp", "tp"),
            P("sp", "tp"),
            P(None, "tp"),
            P(None, "tp", None, None),
            P(None, "tp", None, None),
            P(None, "tp", None, None),
            P(None, "tp", None, None),
            P(None, "tp"),
            P(None, "sp", None, "tp"),
            P("sp", "tp"),
            P(None, "tp"),
            P("tp"),
            P(None, "tp"),
            P(None, "tp"),
            P(None, "tp"),
            P("sp", None, "tp"),
            P("sp", None, "tp"),
            P("sp", None, "tp"),
            P("sp", None),
            P("sp", None),
        ),
        out_specs=P("sp", "tp"),
        check_vma=False,
    )
```
